32 devices in a mesh: tp: 32 (over z, y, x, core).
Axes of the slice: x: 2, y: 2, z: 4, core: 2. Of those that a mesh axis runs over, the one named last changes fastest.
Arguments:
- tokens: bfloat16 [32, 8, 4096], P('tp'), may hold values from -6 to 6
- block_norm_gain: float32 [2, 4096], replicated, may hold values from 0.1 to 1.9
- receptance_weight: bfloat16 [2, 32, 4096, 64], P(None, 'tp'), may hold values from -0.09375 to 0.09375
- key_weight: bfloat16 [2, 32, 4096, 64], P(None, 'tp'), may hold values from -0.09375 to 0.09375
- value_weight: bfloat16 [2, 32, 4096, 64], P(None, 'tp'), may hold values from -0.09375 to 0.09375
- decay_weight: bfloat16 [2, 32, 4096, 64], P(None, 'tp'), may hold values from -0.09375 to 0.09375
- learning_rate_weight: bfloat16 [2, 32, 4096, 64], P(None, 'tp'), may hold values from -0.09375 to 0.09375
- gate_weight: bfloat16 [2, 32, 4096, 64], P(None, 'tp'), may hold values from -0.09375 to 0.09375
- decay_bias_fixed: float32 [2, 2048], replicated, may hold values from -5 to 2
- self_token_weight: float32 [2, 2048], replicated, may hold values from -1.5 to 1.5
- readout_norm_gain: float32 [2, 2048], replicated, may hold values from 0.1 to 1.9
- output_weight: bfloat16 [2, 32, 64, 4096], P(None, 'tp'), may hold values from -0.125 to 0.125
- state: float32 [2, 32, 256, 4096], P(None, 'tp'), may hold values from -3 to 3
Outputs:
- mixed: bfloat16 [32, 8, 4096], P('tp')
- new_state: float32 [2, 32, 256, 4096], P(None, 'tp')
The draws below stay inside these ranges and needn't reach their ends.
All inputs are finite; a program needn't handle non-finite values.
Results may differ from the reference program's by a relative error of at most 0.018.
Values may be sent and summed in bfloat16 or wider, within the bound.
A program may use at most 128 MiB of HBM per device.

```python
import jax
import jax.numpy as jnp
from jax import lax

D = 4096
MIXER_WIDTH = 2048
HEAD_CHANNELS = 64
WINDOW_LAYERS = 2
SEQS = 256
MIXER_HEADS = 32
ROW_BLOCKS = 1
N_TP = 32


def shard_levels(own_key, shape, split, smallest, largest):
    gain = 1.0
    for axis_at, blocks in split:
        steps = jax.random.uniform(jax.random.fold_in(jax.random.fold_in(own_key, 6), axis_at), (blocks,), jnp.float32, smallest / len(split), largest / len(split))
        gain = gain * jnp.repeat(jnp.exp(steps), shape[axis_at] // blocks).reshape((-1,) + (1,) * (len(shape) - 1 - axis_at))
    return gain


def scatter_about(own_key, shape, width, most, pieces=(), dtype=jnp.bfloat16):
    loudness = shard_levels(own_key, shape, pieces, -0.22, 0.18) if pieces else 1.0
    entries = jax.random.normal(own_key, shape, jnp.float32) * width * loudness
    return jnp.minimum(jnp.maximum(entries, -most), most).astype(dtype)


def setup_inputs(seed: int = 0) -> dict:
    streams_of = jax.random.split(jax.random.key(seed), 14)
    tokens = scatter_about(streams_of[0], (N_TP, SEQS // MIXER_HEADS, D // ROW_BLOCKS), 1.0, 6.0, ((0, 32),))
    block_norm_gain = jnp.clip(1.0 + 0.18 * jax.random.normal(streams_of[1], (WINDOW_LAYERS, D), jnp.float32), 0.1, 1.9)
    receptance_weight = scatter_about(streams_of[2], (WINDOW_LAYERS, N_TP, D // ROW_BLOCKS, HEAD_CHANNELS), D ** -0.5, 0.09375, ((1, 32),))
    key_weight = scatter_about(streams_of[3], (WINDOW_LAYERS, N_TP, D // ROW_BLOCKS, HEAD_CHANNELS), D ** -0.5, 0.09375, ((1, 32),))
    value_weight = scatter_about(streams_of[4], (WINDOW_LAYERS, N_TP, D // ROW_BLOCKS, HEAD_CHANNELS), D ** -0.5, 0.09375, ((1, 32),))
    decay_weight = scatter_about(streams_of[5], (WINDOW_LAYERS, N_TP, D // ROW_BLOCKS, HEAD_CHANNELS), D ** -0.5, 0.09375, ((1, 32),))
    learning_rate_weight = scatter_about(streams_of[6], (WINDOW_LAYERS, N_TP, D // ROW_BLOCKS, HEAD_CHANNELS), D ** -0.5, 0.09375, ((1, 32),))
    gate_weight = scatter_about(streams_of[7], (WINDOW_LAYERS, N_TP, D // ROW_BLOCKS, HEAD_CHANNELS), D ** -0.5, 0.09375, ((1, 32),))
    decay_bias_fixed = jnp.clip(jax.random.uniform(streams_of[8], (WINDOW_LAYERS, MIXER_WIDTH), jnp.float32, -5.0, 2.0), -5.0, 2.0)
    self_token_weight = scatter_about(streams_of[9], (WINDOW_LAYERS, MIXER_WIDTH), 0.3, 1.5, (), jnp.float32)
    readout_norm_gain = jnp.clip(1.0 + 0.18 * jax.random.normal(streams_of[10], (WINDOW_LAYERS, MIXER_WIDTH), jnp.float32), 0.1, 1.9)
    output_weight = scatter_about(streams_of[11], (WINDOW_LAYERS, N_TP, HEAD_CHANNELS, D // ROW_BLOCKS), MIXER_WIDTH ** -0.5, 0.125, ((1, 32),))
    state = scatter_about(streams_of[12], (WINDOW_LAYERS, N_TP, SEQS // ROW_BLOCKS, HEAD_CHANNELS * HEAD_CHANNELS), 0.5, 3.0, ((1, 32),), jnp.float32)
    return {"tokens": tokens, "block_norm_gain": block_norm_gain, "receptance_weight": receptance_weight, "key_weight": key_weight, "value_weight": value_weight, "decay_weight": decay_weight, "learning_rate_weight": learning_rate_weight, "gate_weight": gate_weight, "decay_bias_fixed": decay_bias_fixed, "self_token_weight": self_token_weight, "readout_norm_gain": readout_norm_gain, "output_weight": output_weight, "state": state}


RMS_EPS = 1e-06
GROUP_EPS = 0.00064

def recurrent_update(layer_state, receptance_vector, key_vector, value_vector, decay_logits, learning_rate_logits, gate_logits, decay_constant, self_term_scale, head_gain_slice):
    highest = lax.Precision.HIGHEST
    shrink = jnp.exp(-jnp.exp(-jax.nn.softplus(-(decay_constant + decay_logits)) - 0.5))
    rate = jax.nn.sigmoid(learning_rate_logits)
    normed = key_vector * lax.rsqrt(lax.optimization_barrier(jnp.sum(key_vector * key_vector, -1, keepdims=True)) + 1.0)
    removed = jnp.einsum('...ij,...j->...i', layer_state, normed, precision=highest)
    layer_state = layer_state * shrink[..., None, :] - removed[..., :, None] * (normed * rate)[..., None, :] + value_vector[..., :, None] * (key_vector * rate)[..., None, :]
    readout = jnp.einsum('...ij,...j->...i', layer_state, receptance_vector, precision=highest)
    center = lax.optimization_barrier(jnp.mean(readout, -1, keepdims=True))
    spread = lax.optimization_barrier(jnp.mean(jnp.square(readout - center), -1, keepdims=True))
    normed_output = (readout - center) * lax.rsqrt(spread + GROUP_EPS) * head_gain_slice
    self_term = lax.optimization_barrier(jnp.sum(receptance_vector * key_vector * self_term_scale, -1, keepdims=True)) * value_vector
    return (((normed_output + self_term) * jax.nn.sigmoid(gate_logits)).astype(jnp.bfloat16), layer_state)

def reference(tokens, block_norm_gain, receptance_weight, key_weight, value_weight, decay_weight, learning_rate_weight, gate_weight, decay_bias_fixed, self_token_weight, readout_norm_gain, output_weight, state):
    seq_tile = SEQS // MIXER_HEADS
    col_tile = D // ROW_BLOCKS
    seq_block = SEQS // ROW_BLOCKS
    resid = tokens.reshape(MIXER_HEADS, ROW_BLOCKS, seq_tile, col_tile).transpose(0, 2, 1, 3).reshape(SEQS, D)

    def rows_full(weight):
        return weight.reshape(WINDOW_LAYERS, MIXER_HEADS, ROW_BLOCKS, col_tile, HEAD_CHANNELS).transpose(0, 2, 3, 1, 4).reshape(WINDOW_LAYERS, D, MIXER_WIDTH)
    fulls = [rows_full(weight) for weight in (receptance_weight, key_weight, value_weight, decay_weight, learning_rate_weight, gate_weight)]
    out_full = output_weight.reshape(WINDOW_LAYERS, MIXER_HEADS, ROW_BLOCKS, HEAD_CHANNELS, col_tile).transpose(0, 1, 3, 2, 4).reshape(WINDOW_LAYERS, MIXER_WIDTH, D)
    layer_states_stacked = state.reshape(WINDOW_LAYERS, MIXER_HEADS, ROW_BLOCKS, seq_block, HEAD_CHANNELS, HEAD_CHANNELS).transpose(0, 2, 3, 1, 4, 5)
    layer_states_stacked = layer_states_stacked.reshape(WINDOW_LAYERS, SEQS, MIXER_HEADS, HEAD_CHANNELS, HEAD_CHANNELS)
    updated = []
    for layer_index in range(WINDOW_LAYERS):
        wide = resid.astype(jnp.float32)
        scaled = (wide * block_norm_gain[layer_index]).astype(jnp.bfloat16)
        factor = lax.rsqrt(lax.optimization_barrier(jnp.mean(wide * wide, axis=1, keepdims=True)) + RMS_EPS)
        output_pieces = [(jnp.dot(scaled, full[layer_index], preferred_element_type=jnp.float32) * factor).reshape(SEQS, MIXER_HEADS, HEAD_CHANNELS) for full in fulls]
        head_results, layer_state = recurrent_update(layer_states_stacked[layer_index], *output_pieces, decay_bias_fixed[layer_index].reshape(MIXER_HEADS, HEAD_CHANNELS), self_token_weight[layer_index].reshape(MIXER_HEADS, HEAD_CHANNELS), readout_norm_gain[layer_index].reshape(MIXER_HEADS, HEAD_CHANNELS))
        branch = jnp.dot(head_results.reshape(SEQS, MIXER_WIDTH), out_full[layer_index], preferred_element_type=jnp.float32)
        resid = (wide + branch).astype(jnp.bfloat16)
        updated.append(layer_state)
    mixed = resid.reshape(MIXER_HEADS, seq_tile, ROW_BLOCKS, col_tile).transpose(0, 2, 1, 3).reshape(N_TP, seq_tile, col_tile)
    new_state = jnp.stack(updated).reshape(WINDOW_LAYERS, ROW_BLOCKS, seq_block, MIXER_HEADS, HEAD_CHANNELS, HEAD_CHANNELS).transpose(0, 3, 1, 2, 4, 5)
    new_state = new_state.reshape(WINDOW_LAYERS, N_TP, seq_block, HEAD_CHANNELS * HEAD_CHANNELS)
    return (mixed, new_state)
```

```python
import functools

import jax
import jax.numpy as jnp
from jax import lax
from jax.experimental import pallas as pl
from jax.experimental.pallas import tpu as pltpu
from jax.sharding import PartitionSpec as P

D = 4096


RMS_EPS = 1e-06
GROUP_EPS = 0.00064


def swapped(shard, axis, stride):
    return lax.ppermute(shard, axis, [(i, i ^ 1 << stride) for i in range(lax.axis_size(axis))])


def for_sending(shard):

    def short(part):
        return part.astype(jnp.bfloat16) if part.dtype == jnp.float32 else part

    return jax.tree.map(short, shard)


def recurrent_update(
    layer_state,
    receptance_vector,
    key_vector,
    value_vector,
    decay_logits,
    learning_rate_logits,
    gate_logits,
    decay_constant,
    self_term_scale,
    head_gain_slice,
):
    highest = lax.Precision.HIGHEST
    shrink = jnp.exp(-jnp.exp(-jax.nn.softplus(-(decay_constant + decay_logits)) - 0.5))
    rate = jax.nn.sigmoid(learning_rate_logits)
    normed = key_vector * lax.rsqrt(jnp.sum(key_vector * key_vector, -1, keepdims=True) + 1.0)
    removed = jnp.einsum("...ij,...j->...i", layer_state, normed, precision=highest)
    layer_state = (
        layer_state * shrink[..., None, :]
        - removed[..., :, None] * (normed * rate)[..., None, :]
        + value_vector[..., :, None] * (key_vector * rate)[..., None, :]
    )
    readout = jnp.einsum("...ij,...j->...i", layer_state, receptance_vector, precision=highest)
    center = jnp.mean(readout, -1, keepdims=True)
    spread = jnp.mean(jnp.square(readout - center), -1, keepdims=True)
    normed_output = (readout - center) * lax.rsqrt(spread + GROUP_EPS) * head_gain_slice
    self_term = (
        jnp.sum(receptance_vector * key_vector * self_term_scale, -1, keepdims=True) * value_vector
    )
    return (
        ((normed_output + self_term) * jax.nn.sigmoid(gate_logits)).astype(jnp.bfloat16),
        layer_state,
    )


def double_gather(piece, position, first_bit, count, mover):
    for offset in range(count):
        which_bit = first_bit + offset
        partner = mover(piece, which_bit)
        lower_self = position >> which_bit & 1 == 0
        piece = jnp.where(
            lower_self, jnp.concatenate([piece, partner], 0), jnp.concatenate([partner, piece], 0)
        )
    return piece


def halve_sum(members, position, first_bit, count, mover):
    for offset in reversed(range(count)):
        which_bit = first_bit + offset
        upper_self = position >> which_bit & 1 == 1
        sends = tuple(
            (
                jnp.where(
                    upper_self, member[: member.shape[0] // 2], member[member.shape[0] // 2 :]
                )
                for member in members
            )
        )
        keeps = tuple(
            (
                jnp.where(
                    upper_self, member[member.shape[0] // 2 :], member[: member.shape[0] // 2]
                )
                for member in members
            )
        )
        arrived = mover(sends, which_bit)
        members = tuple((kept + got for kept, got in zip(keeps, arrived)))
    return members


def on_device(
    tokens,
    block_norm_gain,
    receptance_weight,
    key_weight,
    value_weight,
    decay_weight,
    learning_rate_weight,
    gate_weight,
    decay_bias_fixed,
    self_token_weight,
    readout_norm_gain,
    output_weight,
    state,
):
    columns_dev = tokens.shape[2]
    row_blocks = D // columns_dev
    low_bits = row_blocks.bit_length() - 1
    head_count = lax.axis_size("tp") // row_blocks
    high_bits = head_count.bit_length() - 1
    position = lax.axis_index("tp")
    head_index = position // row_blocks
    row_block = position % row_blocks
    head_size = receptance_weight.shape[3]
    seq_tile = tokens.shape[1]
    move_rows = lambda payload, which_bit: swapped(payload, "tp", which_bit)
    move_proj = lambda payload, which_bit: swapped(payload, "tp", which_bit)
    move_outs = lambda payload, which_bit: jax.tree.map(
        lambda part, own: part.astype(own.dtype),
        swapped(for_sending(payload), "tp", which_bit),
        payload,
    )
    move_split = lambda payload, which_bit: jax.tree.map(
        lambda part, own: part.astype(own.dtype),
        swapped(for_sending(payload), "tp", which_bit),
        payload,
    )

    def mixer(columns, layer_index):
        gain_cols = lax.dynamic_slice_in_dim(
            block_norm_gain[layer_index], row_block * columns_dev, columns_dev
        )
        wide = columns.astype(jnp.float32)
        scaled = (wide * gain_cols).astype(jnp.bfloat16)
        squares = jnp.sum(wide * wide, axis=1)
        weights = jnp.concatenate(
            [
                receptance_weight[layer_index, 0],
                key_weight[layer_index, 0],
                value_weight[layer_index, 0],
                decay_weight[layer_index, 0],
                learning_rate_weight[layer_index, 0],
                gate_weight[layer_index, 0],
            ],
            axis=1,
        )
        partial_value = jnp.dot(scaled, weights, preferred_element_type=jnp.float32)
        summed, total_sq = halve_sum((partial_value, squares), position, 0, low_bits, move_proj)
        projected = summed * lax.rsqrt(total_sq / D + RMS_EPS)[:, None]
        output_pieces = jnp.split(projected, 6, axis=1)

        def head_columns(table):
            return lax.dynamic_slice_in_dim(table[layer_index], head_index * head_size, head_size)

        layer_state = state[layer_index, 0].reshape(-1, head_size, head_size)
        out_tile, layer_state = recurrent_update(
            layer_state,
            *output_pieces,
            head_columns(decay_bias_fixed),
            head_columns(self_token_weight),
            head_columns(readout_norm_gain)
        )
        out_all = double_gather(out_tile, position, 0, low_bits, move_outs)
        branch = jnp.dot(out_all, output_weight[layer_index, 0], preferred_element_type=jnp.float32)
        return (branch, layer_state.reshape(layer_state.shape[0], head_size * head_size))

    columns = double_gather(tokens[0], position, low_bits, high_bits, move_rows)
    first_branch, first_memory = mixer(columns, 0)
    (tile_sum,) = halve_sum((first_branch,), position, low_bits, high_bits, move_split)
    tile_one = (tokens[0].astype(jnp.float32) + tile_sum).astype(jnp.bfloat16)
    columns = double_gather(tile_one, position, low_bits, high_bits, move_rows)
    second_branch, second_memory = mixer(columns, 1)
    (tile_sum,) = halve_sum((second_branch,), position, low_bits, high_bits, move_split)
    resid_rows = lax.dynamic_slice_in_dim(columns, head_index * seq_tile, seq_tile, 0)
    mixed = (resid_rows.astype(jnp.float32) + tile_sum).astype(jnp.bfloat16)
    new_state = jnp.stack([first_memory, second_memory])[:, None]
    return (mixed[None], new_state)


class Place:
    def __init__(self, n):
        me = lax.axis_index("tp")
        self.n, self.planes = n, n // 8
        self.me = me
        self.i = me % 8
        self.c = me % 2
        self.x = (me // 2) % 2
        self.y = (me // 4) % 2
        self.z = me // 8
        self.sib = self.peer(0, 0, 1)
        self.xn = self.peer(0, 1, 0)
        self.yn = self.peer(1, 0, 0)
        flips = [(1, 1, 0), (1, 1, 1), (1, 0, 0), (1, 0, 1), (0, 1, 0), (0, 1, 1), (0, 0, 1)]
        self.others = [self.peer(*f) for f in flips]
        half = self.planes // 2
        self.near = [k for k in range(1, self.planes) if k != half] + [half]

    def peer(self, dy, dx, dc):
        flip = lambda v, d: 1 - v if d else v
        return self.tile(self.z, flip(self.y, dy), flip(self.x, dx), flip(self.c, dc))

    def tile(self, p, y, x, c):
        return ((p * 2 + y) * 2 + x) * 2 + c

    def plane(self, k):
        return (self.z + k) % self.planes

    def zn(self, k):
        return self.plane(k) * 8 + self.i

    def greet(self):
        barrier = pltpu.get_barrier_semaphore()
        others = self.others + [self.zn(k) for k in self.near]
        for other in others:
            pl.semaphore_signal(
                barrier, inc=1, device_id=(other,), device_id_type=pl.DeviceIdType.MESH
            )
        pl.semaphore_wait(barrier, len(others))


def remote(src, dst, send, recv, to):
    return pltpu.make_async_remote_copy(
        src_ref=src,
        dst_ref=dst,
        send_sem=send,
        recv_sem=recv,
        device_id=(to,),
        device_id_type=pl.DeviceIdType.MESH,
    )


def gather_sends(n):
    planes = n // 8
    return (planes - 1) + 3 * planes + 4 * planes + 2 * planes


class Gather:
    def __init__(self, at, own_ref, full_ref, send, recv_a, recv_b):
        self.at, self.own, self.full = at, own_ref, full_ref
        self.send, self.recv_a, self.recv_b = send, recv_a, recv_b
        half = full_ref.shape[2] // 2
        self.first, self.second = pl.ds(0, half), pl.ds(half, half)
        self.started = []
        self.order = [0] + at.near

    def go(self, src, t, to, cols=None, recv=None):
        dst = self.full.at[t]
        if cols is not None:
            src, dst = src.at[:, cols], dst.at[:, cols]
        recv = self.recv_a if recv is None else recv
        copy = remote(src, dst, self.send.at[len(self.started)], recv.at[t], to)
        copy.start()
        self.started.append(copy)

    def arrived(self, t, cols=None, recv=None):
        dst = self.full.at[t]
        if cols is not None:
            dst = dst.at[:, cols]
        recv = self.recv_a if recv is None else recv
        remote(dst, dst, self.send.at[0], recv.at[t], self.at.sib).wait_recv()

    def start(self):
        at = self.at
        for k in at.near:
            self.go(self.own, at.me, at.zn(k))
        self.go(self.own, at.me, at.xn)
        self.go(self.own, at.me, at.yn)
        self.go(self.own, at.me, at.sib)

    def column(self, k):
        at = self.at
        t = at.zn(k)
        self.arrived(t)
        for to in (at.xn, at.yn, at.sib):
            self.go(self.full.at[t], t, to)

    def spread(self, k):
        at = self.at
        p = at.plane(k)
        t = at.tile(p, at.y, 1 - at.x, at.c)
        self.arrived(t)
        self.go(self.full.at[t], t, at.yn, self.first, self.recv_a)
        self.go(self.full.at[t], t, at.sib)
        t = at.tile(p, 1 - at.y, at.x, at.c)
        self.arrived(t)
        self.go(self.full.at[t], t, at.xn, self.second, self.recv_b)
        self.go(self.full.at[t], t, at.sib)

    def corner(self, k):
        at = self.at
        t = at.tile(at.plane(k), 1 - at.y, 1 - at.x, at.c)
        self.arrived(t, self.first, self.recv_a)
        self.go(self.full.at[t], t, at.sib, self.first, self.recv_a)
        self.arrived(t, self.second, self.recv_b)
        self.go(self.full.at[t], t, at.sib, self.second, self.recv_b)

    def finish(self, k):
        at = self.at
        p = at.plane(k)
        for y in (at.y, 1 - at.y):
            for x in (at.x, 1 - at.x):
                t = at.tile(p, y, x, 1 - at.c)
                if y is not at.y and x is not at.x:
                    self.arrived(t, self.first, self.recv_a)
                    self.arrived(t, self.second, self.recv_b)
                else:
                    self.arrived(t)

    def run(self, batch):
        order = self.order
        for step, k in enumerate(order):
            if step:
                self.column(k)
                self.spread(order[step - 1])
            if step >= 2:
                self.corner(order[step - 2])
        self.spread(order[-1])
        if len(order) > 1:
            self.corner(order[-2])
        self.corner(order[-1])
        for k in order:
            self.finish(k)
            batch(k)

    def drain(self):
        for copy in self.started:
            copy.wait_send()


def lanes(v, times):
    return jnp.concatenate([v] * times, axis=1)


def own_head(ref, layer, head):
    position = lax.axis_index("tp")
    start = pl.multiple_of(position // 2 * (2 * head), 2 * head)
    pair = ref[layer : layer + 1, pl.ds(start, 2 * head)]
    return jnp.where(position % 2 == 0, pair[:, :head], pair[:, head:])


def project(layer, read, columns, gain_ref, w_ref):
    chunk = columns // 8
    acc, squares = None, None
    for j in range(8):
        wide = read(j).astype(jnp.float32)
        cols = slice(j * chunk, (j + 1) * chunk)
        scaled = (wide * gain_ref[layer : layer + 1, cols]).astype(jnp.bfloat16)
        part = lax.dot_general(
            scaled,
            w_ref[layer, :, cols],
            (((1,), (1,)), ((), ())),
            preferred_element_type=jnp.float32,
        )
        square = wide * wide
        folded = square[:, :128]
        for lane in range(128, chunk, 128):
            folded = folded + square[:, lane : lane + 128]
        acc = part if acc is None else acc + part
        squares = folded if squares is None else squares + folded
    mean = jnp.sum(squares, axis=1, keepdims=True) / columns
    return acc * lax.rsqrt(mean + RMS_EPS)


def read_state(proj, heads, state_ref, at_rows, spread_ref):
    bias, self_w, ro_gain = heads
    head = bias.shape[1]
    rows = proj.shape[0]
    flat = state_ref.shape[1]
    chunk = 8 * head
    r, k, v, p, q, g = [proj[:, i * head : (i + 1) * head] for i in range(6)]
    decay = jnp.exp(-jax.nn.sigmoid(bias + p) * jnp.exp(jnp.float32(-0.5)))
    rate = jax.nn.sigmoid(q)
    kn = k * lax.rsqrt(jnp.sum(k * k, axis=1, keepdims=True) + 1.0)
    taken, added = kn * rate, k * rate
    kn_w, u_w = lanes(kn, chunk // head), lanes(decay * r, chunk // head)
    sums = jnp.zeros((2 * rows, head), jnp.float32)
    for at in range(0, flat, chunk):
        s = state_ref[at_rows, at : at + chunk]
        both = jnp.concatenate([s * kn_w, s * u_w], axis=0).astype(jnp.bfloat16)
        sums += lax.dot_general(
            both,
            spread_ref[:head, at : at + chunk],
            (((1,), (1,)), ((), ())),
            preferred_element_type=jnp.float32,
        )
    removed, read = sums[:rows], sums[rows:]
    read = (
        read
        - removed * jnp.sum(taken * r, axis=1, keepdims=True)
        + v * jnp.sum(added * r, axis=1, keepdims=True)
    )
    center = jnp.mean(read, axis=1, keepdims=True)
    off = read - center
    spread = jnp.mean(off * off, axis=1, keepdims=True)
    normed = off * lax.rsqrt(spread + GROUP_EPS) * ro_gain
    own_term = jnp.sum(r * k * self_w, axis=1, keepdims=True) * v
    o = (normed + own_term) * jax.nn.sigmoid(g)
    return o, (removed, v, decay, taken, added)


def write_state(parts, state_ref, at_rows, spread_ref):
    removed, v, decay, taken, added = parts
    rows, head = v.shape
    flat = state_ref.shape[1]
    chunk = 8 * head
    pair = jnp.concatenate([removed, v], axis=0)
    high = pair.astype(jnp.bfloat16)
    low = (pair - high.astype(jnp.float32)).astype(jnp.bfloat16)
    pair = jnp.concatenate([high, low], axis=1)
    decay_w, taken_w, added_w = [lanes(t, chunk // head) for t in (decay, taken, added)]
    for at in range(0, flat, chunk):
        wide = jnp.dot(pair, spread_ref[:, at : at + chunk], preferred_element_type=jnp.float32)
        state_ref[at_rows, at : at + chunk] = (
            state_ref[at_rows, at : at + chunk] * decay_w
            - wide[:rows] * taken_w
            + wide[rows:] * added_w
        )


def fused_kernel(n, own_ref, gain_ref, bias_ref, self_ref, ro_ref, spread_ref, *refs):
    weights, (w_out, state, mixed_ref, new_ref), refs = refs[:6], refs[6:10], refs[10:]
    full_ref, next_ref, joined_ref, wo_ref, o_out, o_in, z_out, z_in, fin, fin_in, mine, *sems = refs
    load, g_send, g_recv_a, g_recv_b, w_send, w_recv, o_send, o_recv, z_send, z_recv, f_send, f_recv = sems
    layers = state.shape[0]
    head = weights[0].shape[2]
    rows, columns = own_ref.shape
    block = columns // 8
    deep = 8 * rows
    f32, bf16 = jnp.float32, jnp.bfloat16

    loads = [[], []]
    state_loads = []
    for layer in range(layers):
        for i, w in enumerate(weights):
            copy = pltpu.make_async_copy(
                w.at[layer, 0], joined_ref.at[layer, pl.ds(i * head, head)], load.at[layer, i]
            )
            copy.start()
            loads[layer].append(copy)
        copy = pltpu.make_async_copy(state.at[layer, 0], new_ref.at[layer, 0], load.at[layer, 6])
        copy.start()
        state_loads.append(copy)

    at = Place(n)
    at.greet()
    own_cols = pl.ds(pl.multiple_of(at.i * block, block), block)
    own_slot = pl.ds(pl.multiple_of(at.i * head, head), head)
    sent = []

    def share_weights(layer):
        for s, to in enumerate(at.others):
            cols = pl.ds(pl.multiple_of(to % 8 * block, block), block)
            copy = remote(
                w_out.at[layer, 0, :, cols],
                wo_ref.at[layer, own_slot],
                w_send.at[layer, s],
                w_recv.at[layer, at.i],
                to,
            )
            copy.start()
            sent.append(copy)
        copy = pltpu.make_async_copy(
            w_out.at[layer, 0, :, own_cols], wo_ref.at[layer, own_slot], load.at[layer, 7]
        )
        copy.start()
        return copy

    def weights_here(layer, own_copy):
        own_copy.wait()
        for other in at.others:
            slot = wo_ref.at[layer, pl.ds(pl.multiple_of(other % 8 * head, head), head)]
            remote(slot, slot, w_send.at[layer, 0], w_recv.at[layer, other % 8], at.sib).wait_recv()

    def mixer(layer, gather, reads, after_last):
        heads = [own_head(t, layer, head) for t in (bias_ref, self_ref, ro_ref)]
        layer_state = new_ref.at[layer, 0]
        waited = []

        def batch(k):
            if not waited:
                for copy in loads[layer]:
                    copy.wait()
                state_loads[layer].wait()
                waited.append(1)
            p = at.plane(k)
            here = pl.ds(pl.multiple_of(p * deep, deep), deep)
            proj = project(layer, functools.partial(reads, p), columns, gain_ref, joined_ref)
            o, parts = read_state(proj, heads, layer_state, here, spread_ref)
            packed = jnp.concatenate([o[: deep // 2], o[deep // 2 :]], axis=1).astype(bf16)
            o_out[layer, k] = packed
            o_in[layer, k, at.i] = packed
            for s, to in enumerate(at.others):
                copy = remote(
                    o_out.at[layer, k],
                    o_in.at[layer, k, at.i],
                    o_send.at[layer, k, s],
                    o_recv.at[layer, k, at.i],
                    to,
                )
                copy.start()
                sent.append(copy)
            write_state(parts, layer_state, here, spread_ref)

        gather.run(batch)
        own_copy = after_last()
        weights_here(layer, own_copy)
        for k in gather.order:
            for other in at.others:
                slot = o_in.at[layer, k, other % 8]
                remote(
                    slot, slot, o_send.at[layer, k, 0], o_recv.at[layer, k, other % 8], at.sib
                ).wait_recv()
            tops, bottoms = [], []
            for j in range(8):
                got = o_in[layer, k, j]
                tops.append(got[:, :head])
                bottoms.append(got[:, head:])
            left = jnp.concatenate(
                [jnp.concatenate(tops, axis=1), jnp.concatenate(bottoms, axis=1)], axis=0
            )
            part = jnp.dot(left, wo_ref[layer], preferred_element_type=f32)
            if k:
                z_out[layer, k] = part.astype(bf16)
                copy = remote(
                    z_out.at[layer, k], z_in.at[layer, k], z_send.at[layer, k], z_recv.at[layer, k], at.zn(k)
                )
                copy.start()
                sent.append(copy)
            else:
                mine[...] = part
        total = mine[...]
        for k in at.near:
            slot = z_in.at[layer, k]
            remote(slot, slot, z_send.at[layer, k], z_recv.at[layer, k], at.sib).wait_recv()
            total = total + z_in[layer, k].astype(f32)
        return total

    full_ref[at.me] = own_ref[...]
    first = Gather(at, own_ref, full_ref, g_send.at[0], g_recv_a.at[0], g_recv_b.at[0])
    first.start()

    def first_reads(p, j):
        tiles = pl.ds(pl.multiple_of(p * 8, 8), 8)
        return full_ref[tiles, :, j * block : (j + 1) * block].reshape(deep, block)

    held = []

    def after_first():
        held.append(share_weights(1))
        return held[0]

    w0 = share_weights(0)
    total = mixer(0, first, first_reads, lambda: (held.append(share_weights(1)), w0)[1])
    mine_tiles = pl.ds(pl.multiple_of(at.z * 8, 8), 8)
    resid = full_ref[mine_tiles, :, own_cols].reshape(deep, block).astype(f32)
    piece = (resid + total).astype(bf16)
    next_ref[at.me] = piece
    second = Gather(at, next_ref.at[at.me], next_ref, g_send.at[1], g_recv_a.at[1], g_recv_b.at[1])
    second.start()
    total = mixer(1, second, lambda p, j: next_ref[p * 8 + j], lambda: held[0])
    done = (next_ref[at.me].astype(f32) + total).astype(bf16)
    fin[...] = done.reshape(8, rows, block)
    fin_in[at.i] = fin[at.i]
    for s, to in enumerate(at.others):
        copy = remote(fin.at[to % 8], fin_in.at[at.i], f_send.at[s], f_recv.at[at.i], to)
        copy.start()
        sent.append(copy)
    for other in at.others:
        slot = fin_in.at[other % 8]
        remote(slot, slot, f_send.at[0], f_recv.at[other % 8], at.sib).wait_recv()
    for j in range(8):
        mixed_ref[:, j * block : (j + 1) * block] = fin_in[j]
    first.drain()
    second.drain()
    for copy in sent:
        copy.wait_send()


def on_device_fast(n, *args):
    tokens, gain, wr, wk, wv, wd, wq, wg, bias, self_w, ro_gain, w_out, state = args
    weights = [jnp.swapaxes(w, 2, 3) for w in (wr, wk, wv, wd, wq, wg)]
    own = tokens[0]
    rows, columns = own.shape
    head = wr.shape[3]
    layers = state.shape[0]
    flat = state.shape[3]
    planes = n // 8
    block, deep = columns // 8, 8 * rows
    bf16, f32 = jnp.bfloat16, jnp.float32
    value_of = jnp.arange(flat) // head
    spread = (jnp.arange(2 * head)[:, None] % head == value_of[None]).astype(bf16)
    vmem, hbm = [pl.BlockSpec(memory_space=m) for m in (pltpu.VMEM, pltpu.HBM)]
    dma = pltpu.SemaphoreType.DMA
    mixed, new_state = pl.pallas_call(
        functools.partial(fused_kernel, n),
        out_shape=(
            jax.ShapeDtypeStruct(own.shape, own.dtype),
            jax.ShapeDtypeStruct(state.shape, state.dtype),
        ),
        in_specs=[vmem] * 6 + [hbm] * 8,
        out_specs=(vmem, vmem),
        scratch_shapes=[
            pltpu.VMEM((n, rows, columns), bf16),
            pltpu.VMEM((n, deep, block), bf16),
            pltpu.VMEM((layers, 6 * head, columns), bf16),
            pltpu.VMEM((layers, 8 * head, block), bf16),
            pltpu.VMEM((layers, planes, deep // 2, 2 * head), bf16),
            pltpu.VMEM((layers, planes, 8, deep // 2, 2 * head), bf16),
            pltpu.VMEM((layers, planes, deep, block), bf16),
            pltpu.VMEM((layers, planes, deep, block), bf16),
            pltpu.VMEM((8, rows, block), bf16),
            pltpu.VMEM((8, rows, block), bf16),
            pltpu.VMEM((deep, block), f32),
            dma((layers, 8)),
            dma((layers, gather_sends(n))),
            dma((layers, n)),
            dma((layers, n)),
            dma((layers, 7)),
            dma((layers, 8)),
            dma((layers, planes, 7)),
            dma((layers, planes, 8)),
            dma((layers, planes)),
            dma((layers, planes)),
            dma((7,)),
            dma((8,)),
        ],
        compiler_params=pltpu.CompilerParams(
            collective_id=0, has_side_effects=True, vmem_limit_bytes=40 << 20
        ),
        cost_estimate=pl.CostEstimate(flops=0, bytes_accessed=50 << 20, transcendentals=0),
    )(own, gain, bias, self_w, ro_gain, spread, *weights, w_out, state)
    return mixed[None], new_state


def pick(n, *args):
    one_block = args[0].shape[2] == args[1].shape[1]
    tiles = args[0].shape[1] % 8 == 0 and args[0].shape[2] % 1024 == 0
    if one_block and tiles and n % 16 == 0 and 2 * args[2].shape[3] % 128 == 0:
        return on_device_fast(n, *args)
    return on_device(*args)


def solution(mesh):
    return jax.shard_map(
        functools.partial(pick, mesh.shape["tp"]),
        mesh=mesh,
        in_specs=(
            P("tp", None, None),
            P(),
            P(None, "tp", None, None),
            P(None, "tp", None, None),
            P(None, "tp", None, None),
            P(None, "tp", None, None),
            P(None, "tp", None, None),
            P(None, "tp", None, None),
            P(),
            P(),
            P(),
            P(None, "tp", None, None),
            P(None, "tp", None, None),
        ),
        out_specs=(P("tp", None, None), P(None, "tp", None, None)),
        check_vma=False,
    )
```

```python
import functools

import jax
import jax.numpy as jnp
from jax import lax
from jax.experimental import pallas as pl
from jax.experimental.pallas import tpu as pltpu
from jax.sharding import PartitionSpec as P

D = 4096


RMS_EPS = 1e-06
GROUP_EPS = 0.00064


def swapped(shard, axis, stride):
    return lax.ppermute(shard, axis, [(i, i ^ 1 << stride) for i in range(lax.axis_size(axis))])


def for_sending(shard):

    def short(part):
        return part.astype(jnp.bfloat16) if part.dtype == jnp.float32 else part

    return jax.tree.map(short, shard)


def recurrent_update(
    layer_state,
    receptance_vector,
    key_vector,
    value_vector,
    decay_logits,
    learning_rate_logits,
    gate_logits,
    decay_constant,
    self_term_scale,
    head_gain_slice,
):
    highest = lax.Precision.HIGHEST
    shrink = jnp.exp(-jnp.exp(-jax.nn.softplus(-(decay_constant + decay_logits)) - 0.5))
    rate = jax.nn.sigmoid(learning_rate_logits)
    normed = key_vector * lax.rsqrt(jnp.sum(key_vector * key_vector, -1, keepdims=True) + 1.0)
    removed = jnp.einsum("...ij,...j->...i", layer_state, normed, precision=highest)
    layer_state = (
        layer_state * shrink[..., None, :]
        - removed[..., :, None] * (normed * rate)[..., None, :]
        + value_vector[..., :, None] * (key_vector * rate)[..., None, :]
    )
    readout = jnp.einsum("...ij,...j->...i", layer_state, receptance_vector, precision=highest)
    center = jnp.mean(readout, -1, keepdims=True)
    spread = jnp.mean(jnp.square(readout - center), -1, keepdims=True)
    normed_output = (readout - center) * lax.rsqrt(spread + GROUP_EPS) * head_gain_slice
    self_term = (
        jnp.sum(receptance_vector * key_vector * self_term_scale, -1, keepdims=True) * value_vector
    )
    return (
        ((normed_output + self_term) * jax.nn.sigmoid(gate_logits)).astype(jnp.bfloat16),
        layer_state,
    )


def double_gather(piece, position, first_bit, count, mover):
    for offset in range(count):
        which_bit = first_bit + offset
        partner = mover(piece, which_bit)
        lower_self = position >> which_bit & 1 == 0
        piece = jnp.where(
            lower_self, jnp.concatenate([piece, partner], 0), jnp.concatenate([partner, piece], 0)
        )
    return piece


def halve_sum(members, position, first_bit, count, mover):
    for offset in reversed(range(count)):
        which_bit = first_bit + offset
        upper_self = position >> which_bit & 1 == 1
        sends = tuple(
            (
                jnp.where(
                    upper_self, member[: member.shape[0] // 2], member[member.shape[0] // 2 :]
                )
                for member in members
            )
        )
        keeps = tuple(
            (
                jnp.where(
                    upper_self, member[member.shape[0] // 2 :], member[: member.shape[0] // 2]
                )
                for member in members
            )
        )
        arrived = mover(sends, which_bit)
        members = tuple((kept + got for kept, got in zip(keeps, arrived)))
    return members


def on_device(
    tokens,
    block_norm_gain,
    receptance_weight,
    key_weight,
    value_weight,
    decay_weight,
    learning_rate_weight,
    gate_weight,
    decay_bias_fixed,
    self_token_weight,
    readout_norm_gain,
    output_weight,
    state,
):
    columns_dev = tokens.shape[2]
    row_blocks = D // columns_dev
    low_bits = row_blocks.bit_length() - 1
    head_count = lax.axis_size("tp") // row_blocks
    high_bits = head_count.bit_length() - 1
    position = lax.axis_index("tp")
    head_index = position // row_blocks
    row_block = position % row_blocks
    head_size = receptance_weight.shape[3]
    seq_tile = tokens.shape[1]
    move_rows = lambda payload, which_bit: swapped(payload, "tp", which_bit)
    move_proj = lambda payload, which_bit: swapped(payload, "tp", which_bit)
    move_outs = lambda payload, which_bit: jax.tree.map(
        lambda part, own: part.astype(own.dtype),
        swapped(for_sending(payload), "tp", which_bit),
        payload,
    )
    move_split = lambda payload, which_bit: jax.tree.map(
        lambda part, own: part.astype(own.dtype),
        swapped(for_sending(payload), "tp", which_bit),
        payload,
    )

    def mixer(columns, layer_index):
        gain_cols = lax.dynamic_slice_in_dim(
            block_norm_gain[layer_index], row_block * columns_dev, columns_dev
        )
        wide = columns.astype(jnp.float32)
        scaled = (wide * gain_cols).astype(jnp.bfloat16)
        squares = jnp.sum(wide * wide, axis=1)
        weights = jnp.concatenate(
            [
                receptance_weight[layer_index, 0],
                key_weight[layer_index, 0],
                value_weight[layer_index, 0],
                decay_weight[layer_index, 0],
                learning_rate_weight[layer_index, 0],
                gate_weight[layer_index, 0],
            ],
            axis=1,
        )
        partial_value = jnp.dot(scaled, weights, preferred_element_type=jnp.float32)
        summed, total_sq = halve_sum((partial_value, squares), position, 0, low_bits, move_proj)
        projected = summed * lax.rsqrt(total_sq / D + RMS_EPS)[:, None]
        output_pieces = jnp.split(projected, 6, axis=1)

        def head_columns(table):
            return lax.dynamic_slice_in_dim(table[layer_index], head_index * head_size, head_size)

        layer_state = state[layer_index, 0].reshape(-1, head_size, head_size)
        out_tile, layer_state = recurrent_update(
            layer_state,
            *output_pieces,
            head_columns(decay_bias_fixed),
            head_columns(self_token_weight),
            head_columns(readout_norm_gain)
        )
        out_all = double_gather(out_tile, position, 0, low_bits, move_outs)
        branch = jnp.dot(out_all, output_weight[layer_index, 0], preferred_element_type=jnp.float32)
        return (branch, layer_state.reshape(layer_state.shape[0], head_size * head_size))

    columns = double_gather(tokens[0], position, low_bits, high_bits, move_rows)
    first_branch, first_memory = mixer(columns, 0)
    (tile_sum,) = halve_sum((first_branch,), position, low_bits, high_bits, move_split)
    tile_one = (tokens[0].astype(jnp.float32) + tile_sum).astype(jnp.bfloat16)
    columns = double_gather(tile_one, position, low_bits, high_bits, move_rows)
    second_branch, second_memory = mixer(columns, 1)
    (tile_sum,) = halve_sum((second_branch,), position, low_bits, high_bits, move_split)
    resid_rows = lax.dynamic_slice_in_dim(columns, head_index * seq_tile, seq_tile, 0)
    mixed = (resid_rows.astype(jnp.float32) + tile_sum).astype(jnp.bfloat16)
    new_state = jnp.stack([first_memory, second_memory])[:, None]
    return (mixed[None], new_state)


class Place:
    def __init__(self, n):
        me = lax.axis_index("tp")
        self.n, self.planes = n, n // 8
        self.me = me
        self.i = me % 8
        self.c = me % 2
        self.x = (me // 2) % 2
        self.y = (me // 4) % 2
        self.z = me // 8
        self.sib = self.peer(0, 0, 1)
        self.xn = self.peer(0, 1, 0)
        self.yn = self.peer(1, 0, 0)
        flips = [(1, 1, 0), (1, 1, 1), (1, 0, 0), (1, 0, 1), (0, 1, 0), (0, 1, 1), (0, 0, 1)]
        self.others = [self.peer(*f) for f in flips]
        self.xyn = self.others[0]
        self.near = list(range(1, self.planes))

    def peer(self, dy, dx, dc):
        flip = lambda v, d: 1 - v if d else v
        return self.tile(self.z, flip(self.y, dy), flip(self.x, dx), flip(self.c, dc))

    def tile(self, p, y, x, c):
        return ((p * 2 + y) * 2 + x) * 2 + c

    def plane(self, k):
        low, high = self.z % 2, self.z // 2
        return 2 * (1 - high if k // 2 else high) + (1 - low if k % 2 else low)

    def zn(self, k):
        return self.plane(k) * 8 + self.i

    def greet(self):
        barrier = pltpu.get_barrier_semaphore()
        others = self.others + [self.zn(k) for k in self.near]
        for other in others:
            pl.semaphore_signal(
                barrier, inc=1, device_id=(other,), device_id_type=pl.DeviceIdType.MESH
            )
        pl.semaphore_wait(barrier, len(others))


def remote(src, dst, send, recv, to):
    return pltpu.make_async_remote_copy(
        src_ref=src,
        dst_ref=dst,
        send_sem=send,
        recv_sem=recv,
        device_id=(to,),
        device_id_type=pl.DeviceIdType.MESH,
    )


def gather_sends(n):
    planes = n // 8
    return (planes - 1) + 7 * planes


class Gather:
    def __init__(self, at, own_ref, full_ref, send, recv):
        self.at, self.own, self.full = at, own_ref, full_ref
        self.send, self.recv = send, recv
        self.started = []

    def go(self, src, t, *tos):
        for to in tos:
            sem = self.send.at[len(self.started)]
            copy = remote(src, self.full.at[t], sem, self.recv.at[t], to)
            copy.start()
            self.started.append(copy)

    def arrived(self, t):
        dst = self.full.at[t]
        remote(dst, dst, self.send.at[0], self.recv.at[t], self.at.sib).wait_recv()

    def start(self):
        at = self.at
        for k in at.near:
            self.go(self.own, at.me, at.zn(k))
        self.go(self.own, at.me, at.xyn, at.xn, at.yn, at.sib)

    def column(self, k):
        at = self.at
        t = at.zn(k)
        self.arrived(t)
        self.go(self.full.at[t], t, at.xyn, at.xn, at.yn, at.sib)

    def across(self, k, c):
        at = self.at
        p = at.plane(k)
        spots = ((at.y, 1 - at.x), (1 - at.y, at.x), (1 - at.y, 1 - at.x))
        return [at.tile(p, y, x, c) for y, x in spots]

    def sides(self, k):
        for t in self.across(k, self.at.c):
            self.arrived(t)
            self.go(self.full.at[t], t, self.at.sib)

    def finish(self, k):
        at = self.at
        self.arrived(at.tile(at.plane(k), at.y, at.x, 1 - at.c))
        for t in self.across(k, 1 - at.c):
            self.arrived(t)

    def drain(self):
        for copy in self.started:
            copy.wait_send()


def lanes(v, times):
    return jnp.concatenate([v] * times, axis=1)


def own_head(ref, layer, head):
    position = lax.axis_index("tp")
    start = pl.multiple_of(position // 2 * (2 * head), 2 * head)
    pair = ref[layer : layer + 1, pl.ds(start, 2 * head)]
    return jnp.where(position % 2 == 0, pair[:, :head], pair[:, head:])


def project(layer, read, columns, gain_ref, w_ref):
    chunk = columns // 8
    acc, squares = None, None
    for j in range(8):
        wide = read(j).astype(jnp.float32)
        cols = slice(j * chunk, (j + 1) * chunk)
        scaled = (wide * gain_ref[layer : layer + 1, cols]).astype(jnp.bfloat16)
        part = lax.dot_general(
            scaled,
            w_ref[layer, :, cols],
            (((1,), (1,)), ((), ())),
            preferred_element_type=jnp.float32,
        )
        square = wide * wide
        folded = square[:, :128]
        for lane in range(128, chunk, 128):
            folded = folded + square[:, lane : lane + 128]
        acc = part if acc is None else acc + part
        squares = folded if squares is None else squares + folded
    mean = jnp.sum(squares, axis=1, keepdims=True) / columns
    return acc * lax.rsqrt(mean + RMS_EPS)


def read_state(proj, heads, state_ref, at_rows, spread_ref):
    bias, self_w, ro_gain = heads
    head = bias.shape[1]
    rows = proj.shape[0]
    flat = state_ref.shape[1]
    chunk = 8 * head
    r, k, v, p, q, g = [proj[:, i * head : (i + 1) * head] for i in range(6)]
    decay = jnp.exp(-jax.nn.sigmoid(bias + p) * jnp.exp(jnp.float32(-0.5)))
    rate = jax.nn.sigmoid(q)
    kn = k * lax.rsqrt(jnp.sum(k * k, axis=1, keepdims=True) + 1.0)
    taken, added = kn * rate, k * rate
    kn_w, u_w = lanes(kn, chunk // head), lanes(decay * r, chunk // head)
    sums = jnp.zeros((2 * rows, head), jnp.float32)
    for at in range(0, flat, chunk):
        s = state_ref[at_rows, at : at + chunk]
        both = jnp.concatenate([s * kn_w, s * u_w], axis=0).astype(jnp.bfloat16)
        sums += lax.dot_general(
            both,
            spread_ref[:head, at : at + chunk],
            (((1,), (1,)), ((), ())),
            preferred_element_type=jnp.float32,
        )
    removed, read = sums[:rows], sums[rows:]
    read = (
        read
        - removed * jnp.sum(taken * r, axis=1, keepdims=True)
        + v * jnp.sum(added * r, axis=1, keepdims=True)
    )
    center = jnp.mean(read, axis=1, keepdims=True)
    off = read - center
    spread = jnp.mean(off * off, axis=1, keepdims=True)
    normed = off * lax.rsqrt(spread + GROUP_EPS) * ro_gain
    own_term = jnp.sum(r * k * self_w, axis=1, keepdims=True) * v
    o = (normed + own_term) * jax.nn.sigmoid(g)
    return o, (removed, v, decay, taken, added)


def write_state(parts, state_ref, at_rows, spread_ref):
    removed, v, decay, taken, added = parts
    rows, head = v.shape
    flat = state_ref.shape[1]
    chunk = 8 * head
    pair = jnp.concatenate([removed, v], axis=0)
    high = pair.astype(jnp.bfloat16)
    low = (pair - high.astype(jnp.float32)).astype(jnp.bfloat16)
    pair = jnp.concatenate([high, low], axis=1)
    decay_w, taken_w, added_w = [lanes(t, chunk // head) for t in (decay, taken, added)]
    for at in range(0, flat, chunk):
        wide = jnp.dot(pair, spread_ref[:, at : at + chunk], preferred_element_type=jnp.float32)
        state_ref[at_rows, at : at + chunk] = (
            state_ref[at_rows, at : at + chunk] * decay_w
            - wide[:rows] * taken_w
            + wide[rows:] * added_w
        )


def put_spread(spread_ref, head):
    chunk = 8 * head
    shape = (spread_ref.shape[0], chunk)
    lane = lax.broadcasted_iota(jnp.int32, shape, 1) // head
    row = lax.broadcasted_iota(jnp.int32, shape, 0) % head
    for at in range(0, spread_ref.shape[1], chunk):
        hit = row == lane + at // head
        spread_ref[:, at : at + chunk] = jnp.where(hit, 1.0, 0.0).astype(jnp.bfloat16)


def fused_kernel(n, own_hbm, gain_hbm, bias_hbm, self_hbm, ro_hbm, *refs):
    weights, (w_out, state, mixed_ref, new_ref), refs = refs[:6], refs[6:10], refs[10:]
    spread_ref, gain_ref, bias_ref, self_ref, ro_ref, early, *refs = refs
    full_ref, next_ref, joined_ref, wo_ref, o_out, o_in, z_out, z_in, fin, fin_in, mine, *sems = refs
    load, g_send, g_recv, w_send, w_recv, o_send, o_recv, z_send, z_recv, f_send, f_recv = sems
    layers = state.shape[0]
    head = weights[0].shape[2]
    rows, columns = own_hbm.shape
    block = columns // 8
    deep = 8 * rows
    f32, bf16 = jnp.float32, jnp.bfloat16
    at = Place(n)

    def fetch(i, src, dst):
        copy = pltpu.make_async_copy(src, dst, early.at[i])
        copy.start()
        return copy

    own_load = fetch(0, own_hbm, full_ref.at[at.me])
    tables = [
        fetch(1, gain_hbm, gain_ref),
        fetch(2, bias_hbm, bias_ref),
        fetch(3, self_hbm, self_ref),
        fetch(4, ro_hbm, ro_ref),
    ]
    loads = [tables] + [[] for _ in range(1, layers)]
    state_loads = []
    for layer in range(layers):
        for i, w in enumerate(weights):
            copy = pltpu.make_async_copy(
                w.at[layer, 0], joined_ref.at[layer, pl.ds(i * head, head)], load.at[layer, i]
            )
            copy.start()
            loads[layer].append(copy)
        copy = pltpu.make_async_copy(state.at[layer, 0], new_ref.at[layer, 0], load.at[layer, 6])
        copy.start()
        state_loads.append(copy)

    at.greet()
    own_cols = pl.ds(pl.multiple_of(at.i * block, block), block)
    own_slot = pl.ds(pl.multiple_of(at.i * head, head), head)
    sent, own_weights = [], []

    def share_weights(layer):
        for s, to in enumerate(at.others):
            cols = pl.ds(pl.multiple_of(to % 8 * block, block), block)
            copy = remote(
                w_out.at[layer, 0, :, cols],
                wo_ref.at[layer, own_slot],
                w_send.at[layer, s],
                w_recv.at[layer, at.i],
                to,
            )
            copy.start()
            sent.append(copy)
        copy = pltpu.make_async_copy(
            w_out.at[layer, 0, :, own_cols], wo_ref.at[layer, own_slot], load.at[layer, 7]
        )
        copy.start()
        own_weights.append(copy)

    def weights_here(layer):
        own_weights[layer].wait()
        for other in at.others:
            slot = wo_ref.at[layer, pl.ds(pl.multiple_of(other % 8 * head, head), head)]
            remote(slot, slot, w_send.at[layer, 0], w_recv.at[layer, other % 8], at.sib).wait_recv()

    def mixer(layer, gather, reads, share_early, share_late):
        heads = []
        layer_state = new_ref.at[layer, 0]
        zero, a, b, c = range(at.planes)
        held = {}

        def here(k):
            return pl.ds(pl.multiple_of(at.plane(k) * deep, deep), deep)

        def projected(k):
            gather.finish(k)
            if not heads:
                for copy in loads[layer]:
                    copy.wait()
                heads.extend(own_head(t, layer, head) for t in (bias_ref, self_ref, ro_ref))
            held[k] = project(
                layer, functools.partial(reads, at.plane(k)), columns, gain_ref, joined_ref
            )

        def mixed_rows(k):
            if k == zero:
                state_loads[layer].wait()
            o, held[k] = read_state(held[k], heads, layer_state, here(k), spread_ref)
            packed = jnp.concatenate([o[: deep // 2], o[deep // 2 :]], axis=1).astype(bf16)
            o_out[layer, k] = packed
            o_in[layer, k, at.i] = packed
            for s, to in enumerate(at.others):
                copy = remote(
                    o_out.at[layer, k],
                    o_in.at[layer, k, at.i],
                    o_send.at[layer, k, s],
                    o_recv.at[layer, k, at.i],
                    to,
                )
                copy.start()
                sent.append(copy)

        def update(k):
            write_state(held[k], layer_state, here(k), spread_ref)

        def emit(k):
            for other in at.others:
                slot = o_in.at[layer, k, other % 8]
                remote(
                    slot, slot, o_send.at[layer, k, 0], o_recv.at[layer, k, other % 8], at.sib
                ).wait_recv()
            tops, bottoms = [], []
            for j in range(8):
                got = o_in[layer, k, j]
                tops.append(got[:, :head])
                bottoms.append(got[:, head:])
            left = jnp.concatenate(
                [jnp.concatenate(tops, axis=1), jnp.concatenate(bottoms, axis=1)], axis=0
            )
            part = jnp.dot(left, wo_ref[layer], preferred_element_type=f32)
            if k == zero:
                mine[...] = part
                return
            z_out[layer, k] = part.astype(bf16)
            copy = remote(
                z_out.at[layer, k], z_in.at[layer, k], z_send.at[layer, k], z_recv.at[layer, k], at.zn(k)
            )
            copy.start()
            sent.append(copy)

        gather.column(a)
        gather.sides(zero)
        gather.column(b)
        projected(zero)
        gather.column(c)
        share_early()
        gather.sides(a)
        mixed_rows(zero)
        projected(a)
        gather.sides(b)
        mixed_rows(a)
        gather.sides(c)
        projected(b)
        mixed_rows(b)
        projected(c)
        mixed_rows(c)
        share_late()
        update(zero)
        weights_here(layer)
        emit(a)
        emit(b)
        emit(zero)
        update(a)
        update(b)
        emit(c)
        update(c)
        total = mine[...]
        for k in at.near:
            slot = z_in.at[layer, k]
            remote(slot, slot, z_send.at[layer, k], z_recv.at[layer, k], at.sib).wait_recv()
            total = total + z_in[layer, k].astype(f32)
        return total

    own_load.wait()
    first = Gather(at, full_ref.at[at.me], full_ref, g_send.at[0], g_recv.at[0])
    first.start()

    def first_reads(p, j):
        tiles = pl.ds(pl.multiple_of(p * 8, 8), 8)
        return full_ref[tiles, :, j * block : (j + 1) * block].reshape(deep, block)

    put_spread(spread_ref, head)
    total = mixer(
        0, first, first_reads, functools.partial(share_weights, 0), functools.partial(share_weights, 1)
    )
    mine_tiles = pl.ds(pl.multiple_of(at.z * 8, 8), 8)
    resid = full_ref[mine_tiles, :, own_cols].reshape(deep, block).astype(f32)
    piece = (resid + total).astype(bf16)
    next_ref[at.me] = piece
    second = Gather(at, next_ref.at[at.me], next_ref, g_send.at[1], g_recv.at[1])
    second.start()
    nothing = lambda: None
    total = mixer(1, second, lambda p, j: next_ref[p * 8 + j], nothing, nothing)
    done = (next_ref[at.me].astype(f32) + total).astype(bf16)
    fin[...] = done.reshape(8, rows, block)
    fin_in[at.i] = fin[at.i]
    for s, to in enumerate(at.others):
        copy = remote(fin.at[to % 8], fin_in.at[at.i], f_send.at[s], f_recv.at[at.i], to)
        copy.start()
        sent.append(copy)
    for other in at.others:
        slot = fin_in.at[other % 8]
        remote(slot, slot, f_send.at[0], f_recv.at[other % 8], at.sib).wait_recv()
    for j in range(8):
        mixed_ref[:, j * block : (j + 1) * block] = fin_in[j]
    first.drain()
    second.drain()
    for copy in sent:
        copy.wait_send()


def on_device_fast(n, *args):
    tokens, gain, wr, wk, wv, wd, wq, wg, bias, self_w, ro_gain, w_out, state = args
    weights = [jnp.swapaxes(w, 2, 3) for w in (wr, wk, wv, wd, wq, wg)]
    own = tokens[0]
    rows, columns = own.shape
    head = wr.shape[3]
    layers = state.shape[0]
    flat = state.shape[3]
    planes = n // 8
    block, deep = columns // 8, 8 * rows
    bf16, f32 = jnp.bfloat16, jnp.float32
    vmem, hbm = [pl.BlockSpec(memory_space=m) for m in (pltpu.VMEM, pltpu.HBM)]
    dma = pltpu.SemaphoreType.DMA
    stay = lambda a: pltpu.with_memory_space_constraint(a, pltpu.HBM)
    operands = [own, gain, bias, self_w, ro_gain, *weights, w_out, state]
    mixed, new_state = pl.pallas_call(
        functools.partial(fused_kernel, n),
        out_shape=(
            jax.ShapeDtypeStruct(own.shape, own.dtype),
            pltpu.VMEM(state.shape, state.dtype),
        ),
        in_specs=[hbm] * len(operands),
        out_specs=(vmem, vmem),
        scratch_shapes=[
            pltpu.VMEM((2 * head, flat), bf16),
            *[pltpu.VMEM(t.shape, t.dtype) for t in (gain, bias, self_w, ro_gain)],
            dma((5,)),
            pltpu.VMEM((n, rows, columns), bf16),
            pltpu.VMEM((n, deep, block), bf16),
            pltpu.VMEM((layers, 6 * head, columns), bf16),
            pltpu.VMEM((layers, 8 * head, block), bf16),
            pltpu.VMEM((layers, planes, deep // 2, 2 * head), bf16),
            pltpu.VMEM((layers, planes, 8, deep // 2, 2 * head), bf16),
            pltpu.VMEM((layers, planes, deep, block), bf16),
            pltpu.VMEM((layers, planes, deep, block), bf16),
            pltpu.VMEM((8, rows, block), bf16),
            pltpu.VMEM((8, rows, block), bf16),
            pltpu.VMEM((deep, block), f32),
            dma((layers, 8)),
            dma((layers, gather_sends(n))),
            dma((layers, n)),
            dma((layers, 7)),
            dma((layers, 8)),
            dma((layers, planes, 7)),
            dma((layers, planes, 8)),
            dma((layers, planes)),
            dma((layers, planes)),
            dma((7,)),
            dma((8,)),
        ],
        compiler_params=pltpu.CompilerParams(
            collective_id=0, has_side_effects=True, vmem_limit_bytes=40 << 20
        ),
        cost_estimate=pl.CostEstimate(flops=0, bytes_accessed=50 << 20, transcendentals=0),
    )(*[stay(o) for o in operands])
    return mixed[None], new_state


def pick(n, *args):
    one_block = args[0].shape[2] == args[1].shape[1]
    tiles = args[0].shape[1] % 8 == 0 and args[0].shape[2] % 1024 == 0
    if one_block and tiles and n // 8 == 4 and 2 * args[2].shape[3] % 128 == 0:
        return on_device_fast(n, *args)
    return on_device(*args)


def solution(mesh):
    return jax.shard_map(
        functools.partial(pick, mesh.shape["tp"]),
        mesh=mesh,
        in_specs=(
            P("tp", None, None),
            P(),
            P(None, "tp", None, None),
            P(None, "tp", None, None),
            P(None, "tp", None, None),
            P(None, "tp", None, None),
            P(None, "tp", None, None),
            P(None, "tp", None, None),
            P(),
            P(),
            P(),
            P(None, "tp", None, None),
            P(None, "tp", None, None),
        ),
        out_specs=(P("tp", None, None), P(None, "tp", None, None)),
        check_vma=False,
    )
```

```python
import functools

import jax
import jax.numpy as jnp
from jax import lax
from jax.experimental import pallas as pl
from jax.experimental.pallas import tpu as pltpu
from jax.sharding import PartitionSpec as P

D = 4096


RMS_EPS = 1e-06
GROUP_EPS = 0.00064


def swapped(shard, axis, stride):
    return lax.ppermute(shard, axis, [(i, i ^ 1 << stride) for i in range(lax.axis_size(axis))])


def for_sending(shard):

    def short(part):
        return part.astype(jnp.bfloat16) if part.dtype == jnp.float32 else part

    return jax.tree.map(short, shard)


def recurrent_update(
    layer_state,
    receptance_vector,
    key_vector,
    value_vector,
    decay_logits,
    learning_rate_logits,
    gate_logits,
    decay_constant,
    self_term_scale,
    head_gain_slice,
):
    highest = lax.Precision.HIGHEST
    shrink = jnp.exp(-jnp.exp(-jax.nn.softplus(-(decay_constant + decay_logits)) - 0.5))
    rate = jax.nn.sigmoid(learning_rate_logits)
    normed = key_vector * lax.rsqrt(jnp.sum(key_vector * key_vector, -1, keepdims=True) + 1.0)
    removed = jnp.einsum("...ij,...j->...i", layer_state, normed, precision=highest)
    layer_state = (
        layer_state * shrink[..., None, :]
        - removed[..., :, None] * (normed * rate)[..., None, :]
        + value_vector[..., :, None] * (key_vector * rate)[..., None, :]
    )
    readout = jnp.einsum("...ij,...j->...i", layer_state, receptance_vector, precision=highest)
    center = jnp.mean(readout, -1, keepdims=True)
    spread = jnp.mean(jnp.square(readout - center), -1, keepdims=True)
    normed_output = (readout - center) * lax.rsqrt(spread + GROUP_EPS) * head_gain_slice
    self_term = (
        jnp.sum(receptance_vector * key_vector * self_term_scale, -1, keepdims=True) * value_vector
    )
    return (
        ((normed_output + self_term) * jax.nn.sigmoid(gate_logits)).astype(jnp.bfloat16),
        layer_state,
    )


def double_gather(piece, position, first_bit, count, mover):
    for offset in range(count):
        which_bit = first_bit + offset
        partner = mover(piece, which_bit)
        lower_self = position >> which_bit & 1 == 0
        piece = jnp.where(
            lower_self, jnp.concatenate([piece, partner], 0), jnp.concatenate([partner, piece], 0)
        )
    return piece


def halve_sum(members, position, first_bit, count, mover):
    for offset in reversed(range(count)):
        which_bit = first_bit + offset
        upper_self = position >> which_bit & 1 == 1
        sends = tuple(
            (
                jnp.where(
                    upper_self, member[: member.shape[0] // 2], member[member.shape[0] // 2 :]
                )
                for member in members
            )
        )
        keeps = tuple(
            (
                jnp.where(
                    upper_self, member[member.shape[0] // 2 :], member[: member.shape[0] // 2]
                )
                for member in members
            )
        )
        arrived = mover(sends, which_bit)
        members = tuple((kept + got for kept, got in zip(keeps, arrived)))
    return members


def on_device(
    tokens,
    block_norm_gain,
    receptance_weight,
    key_weight,
    value_weight,
    decay_weight,
    learning_rate_weight,
    gate_weight,
    decay_bias_fixed,
    self_token_weight,
    readout_norm_gain,
    output_weight,
    state,
):
    columns_dev = tokens.shape[2]
    row_blocks = D // columns_dev
    low_bits = row_blocks.bit_length() - 1
    head_count = lax.axis_size("tp") // row_blocks
    high_bits = head_count.bit_length() - 1
    position = lax.axis_index("tp")
    head_index = position // row_blocks
    row_block = position % row_blocks
    head_size = receptance_weight.shape[3]
    seq_tile = tokens.shape[1]
    move_rows = lambda payload, which_bit: swapped(payload, "tp", which_bit)
    move_proj = lambda payload, which_bit: swapped(payload, "tp", which_bit)
    move_outs = lambda payload, which_bit: jax.tree.map(
        lambda part, own: part.astype(own.dtype),
        swapped(for_sending(payload), "tp", which_bit),
        payload,
    )
    move_split = lambda payload, which_bit: jax.tree.map(
        lambda part, own: part.astype(own.dtype),
        swapped(for_sending(payload), "tp", which_bit),
        payload,
    )

    def mixer(columns, layer_index):
        gain_cols = lax.dynamic_slice_in_dim(
            block_norm_gain[layer_index], row_block * columns_dev, columns_dev
        )
        wide = columns.astype(jnp.float32)
        scaled = (wide * gain_cols).astype(jnp.bfloat16)
        squares = jnp.sum(wide * wide, axis=1)
        weights = jnp.concatenate(
            [
                receptance_weight[layer_index, 0],
                key_weight[layer_index, 0],
                value_weight[layer_index, 0],
                decay_weight[layer_index, 0],
                learning_rate_weight[layer_index, 0],
                gate_weight[layer_index, 0],
            ],
            axis=1,
        )
        partial_value = jnp.dot(scaled, weights, preferred_element_type=jnp.float32)
        summed, total_sq = halve_sum((partial_value, squares), position, 0, low_bits, move_proj)
        projected = summed * lax.rsqrt(total_sq / D + RMS_EPS)[:, None]
        output_pieces = jnp.split(projected, 6, axis=1)

        def head_columns(table):
            return lax.dynamic_slice_in_dim(table[layer_index], head_index * head_size, head_size)

        layer_state = state[layer_index, 0].reshape(-1, head_size, head_size)
        out_tile, layer_state = recurrent_update(
            layer_state,
            *output_pieces,
            head_columns(decay_bias_fixed),
            head_columns(self_token_weight),
            head_columns(readout_norm_gain)
        )
        out_all = double_gather(out_tile, position, 0, low_bits, move_outs)
        branch = jnp.dot(out_all, output_weight[layer_index, 0], preferred_element_type=jnp.float32)
        return (branch, layer_state.reshape(layer_state.shape[0], head_size * head_size))

    columns = double_gather(tokens[0], position, low_bits, high_bits, move_rows)
    first_branch, first_memory = mixer(columns, 0)
    (tile_sum,) = halve_sum((first_branch,), position, low_bits, high_bits, move_split)
    tile_one = (tokens[0].astype(jnp.float32) + tile_sum).astype(jnp.bfloat16)
    columns = double_gather(tile_one, position, low_bits, high_bits, move_rows)
    second_branch, second_memory = mixer(columns, 1)
    (tile_sum,) = halve_sum((second_branch,), position, low_bits, high_bits, move_split)
    resid_rows = lax.dynamic_slice_in_dim(columns, head_index * seq_tile, seq_tile, 0)
    mixed = (resid_rows.astype(jnp.float32) + tile_sum).astype(jnp.bfloat16)
    new_state = jnp.stack([first_memory, second_memory])[:, None]
    return (mixed[None], new_state)


class Place:
    def __init__(self, n):
        me = lax.axis_index("tp")
        self.n, self.planes = n, n // 8
        self.me = me
        self.i = me % 8
        self.c = me % 2
        self.x = (me // 2) % 2
        self.y = (me // 4) % 2
        self.z = me // 8
        self.sib = self.peer(0, 0, 1)
        self.xn = self.peer(0, 1, 0)
        self.yn = self.peer(1, 0, 0)
        flips = [(1, 1, 0), (1, 1, 1), (1, 0, 0), (1, 0, 1), (0, 1, 0), (0, 1, 1), (0, 0, 1)]
        self.others = [self.peer(*f) for f in flips]
        self.xyn = self.others[0]
        self.near = [1, 3, 2]

    def peer(self, dy, dx, dc):
        flip = lambda v, d: 1 - v if d else v
        return self.tile(self.z, flip(self.y, dy), flip(self.x, dx), flip(self.c, dc))

    def tile(self, p, y, x, c):
        return ((p * 2 + y) * 2 + x) * 2 + c

    def plane(self, k):
        low, high = self.z % 2, self.z // 2
        return 2 * (1 - high if k // 2 else high) + (1 - low if k % 2 else low)

    def zn(self, k):
        return self.plane(k) * 8 + self.i

    def greet(self):
        barrier = pltpu.get_barrier_semaphore()
        others = self.others + [self.zn(k) for k in self.near]
        for other in others:
            pl.semaphore_signal(
                barrier, inc=1, device_id=(other,), device_id_type=pl.DeviceIdType.MESH
            )
        pl.semaphore_wait(barrier, len(others))


def remote(src, dst, send, recv, to):
    return pltpu.make_async_remote_copy(
        src_ref=src,
        dst_ref=dst,
        send_sem=send,
        recv_sem=recv,
        device_id=(to,),
        device_id_type=pl.DeviceIdType.MESH,
    )


GATHER_SENDS = 3 + 4 + 1 + 2 * 4 + 6 + 3 * 3


class Gather:
    def __init__(self, at, own_ref, full_ref, send, recv):
        self.at, self.own, self.full = at, own_ref, full_ref
        self.send, self.recv = send, recv
        self.inner = at.z % 2 != at.z // 2

    def spot(self, k, i):
        return k * 4 + i

    def go(self, src, t, spot, *tos):
        for to in tos:
            remote(src, self.full.at[t], self.send.at[0], self.recv.at[spot], to).start()

    def arrived(self, spot, tiles=1):
        dst = self.full.at[pl.ds(0, tiles)]
        remote(dst, dst, self.send.at[0], self.recv.at[spot], self.at.sib).wait_recv()

    def cross(self, k, src, t):
        at = self.at
        for i, to in enumerate((at.xyn, at.xn, at.yn)):
            self.go(src, t, self.spot(k, i), to)
        self.to_sib(k, src, t)

    def to_sib(self, k, src, t):
        self.go(src, t, self.spot(k, 3), self.at.sib)

    def along(self, k):
        return 4 * self.at.planes + k - 1

    def start(self):
        at = self.at
        for k in (1, 3):
            self.go(self.own, at.me, self.along(k), at.zn(k))

        @pl.when(jnp.logical_not(self.inner))
        def _():
            self.go(self.own, at.me, self.along(2), at.zn(2))

        self.cross(0, self.own, at.me)

    def adjacent(self):
        t = self.at.zn(1)
        self.arrived(self.along(1))
        self.to_sib(1, self.full.at[t], t)

    def column(self, k):
        t = self.at.zn(k)
        self.arrived(self.along(k))
        self.cross(k, self.full.at[t], t)

    def middle_early(self):
        @pl.when(self.inner)
        def _():
            t = self.at.zn(3)
            self.arrived(self.along(3))
            self.go(self.full.at[t], t, self.along(2), self.at.zn(1))
            self.cross(3, self.full.at[t], t)

    def middle_late(self):
        @pl.when(jnp.logical_not(self.inner))
        def _():
            self.column(3)

    def sides(self, k):
        at = self.at
        p = at.plane(k)
        spots = ((1 - at.y, 1 - at.x), (at.y, 1 - at.x), (1 - at.y, at.x))
        for i in (1, 2, 0):
            y, x = spots[i]
            t = at.tile(p, y, x, at.c)
            self.arrived(self.spot(k, i))
            if not k:
                self.go(self.full.at[t], t, self.spot(1, i), at.zn(1))
            self.to_sib(k, self.full.at[t], t)

    def finish(self, k):
        self.arrived(self.spot(k, 3), 4)

    def drain(self):
        dst = self.full.at[pl.ds(0, GATHER_SENDS)]
        remote(dst, dst, self.send.at[0], self.recv.at[0], self.at.sib).wait_send()


def lanes(v, times):
    return jnp.concatenate([v] * times, axis=1)


def own_head(ref, layer, head):
    position = lax.axis_index("tp")
    start = pl.multiple_of(position // 2 * (2 * head), 2 * head)
    pair = ref[layer : layer + 1, pl.ds(start, 2 * head)]
    return jnp.where(position % 2 == 0, pair[:, :head], pair[:, head:])


def project(layer, read, columns, gain_ref, w_ref):
    chunk = columns // 8
    acc, squares = None, None
    for j in range(8):
        wide = read(j).astype(jnp.float32)
        cols = slice(j * chunk, (j + 1) * chunk)
        scaled = (wide * gain_ref[layer : layer + 1, cols]).astype(jnp.bfloat16)
        part = lax.dot_general(
            scaled,
            w_ref[layer, :, cols],
            (((1,), (1,)), ((), ())),
            preferred_element_type=jnp.float32,
        )
        square = wide * wide
        folded = square[:, :128]
        for lane in range(128, chunk, 128):
            folded = folded + square[:, lane : lane + 128]
        acc = part if acc is None else acc + part
        squares = folded if squares is None else squares + folded
    mean = jnp.sum(squares, axis=1, keepdims=True) / columns
    return acc * lax.rsqrt(mean + RMS_EPS)


def read_state(proj, heads, state_ref, at_rows, spread_ref):
    bias, self_w, ro_gain = heads
    head = bias.shape[1]
    rows = proj.shape[0]
    flat = state_ref.shape[1]
    chunk = 8 * head
    r, k, v, p, q, g = [proj[:, i * head : (i + 1) * head] for i in range(6)]
    decay = jnp.exp(-jax.nn.sigmoid(bias + p) * jnp.exp(jnp.float32(-0.5)))
    rate = jax.nn.sigmoid(q)
    kn = k * lax.rsqrt(jnp.sum(k * k, axis=1, keepdims=True) + 1.0)
    taken, added = kn * rate, k * rate
    kn_w, u_w = lanes(kn, chunk // head), lanes(decay * r, chunk // head)
    sums = jnp.zeros((2 * rows, head), jnp.float32)
    for at in range(0, flat, chunk):
        s = state_ref[at_rows, at : at + chunk]
        both = jnp.concatenate([s * kn_w, s * u_w], axis=0).astype(jnp.bfloat16)
        sums += lax.dot_general(
            both,
            spread_ref[:head, at : at + chunk],
            (((1,), (1,)), ((), ())),
            preferred_element_type=jnp.float32,
        )
    removed, read = sums[:rows], sums[rows:]
    read = (
        read
        - removed * jnp.sum(taken * r, axis=1, keepdims=True)
        + v * jnp.sum(added * r, axis=1, keepdims=True)
    )
    center = jnp.mean(read, axis=1, keepdims=True)
    off = read - center
    spread = jnp.mean(off * off, axis=1, keepdims=True)
    normed = off * lax.rsqrt(spread + GROUP_EPS) * ro_gain
    own_term = jnp.sum(r * k * self_w, axis=1, keepdims=True) * v
    o = (normed + own_term) * jax.nn.sigmoid(g)
    return o, (removed, v, decay, taken, added)


def write_state(parts, state_ref, at_rows, spread_ref):
    removed, v, decay, taken, added = parts
    rows, head = v.shape
    flat = state_ref.shape[1]
    chunk = 8 * head
    pair = jnp.concatenate([removed, v], axis=0)
    high = pair.astype(jnp.bfloat16)
    low = (pair - high.astype(jnp.float32)).astype(jnp.bfloat16)
    pair = jnp.concatenate([high, low], axis=1)
    decay_w, taken_w, added_w = [lanes(t, chunk // head) for t in (decay, taken, added)]
    for at in range(0, flat, chunk):
        wide = jnp.dot(pair, spread_ref[:, at : at + chunk], preferred_element_type=jnp.float32)
        state_ref[at_rows, at : at + chunk] = (
            state_ref[at_rows, at : at + chunk] * decay_w
            - wide[:rows] * taken_w
            + wide[rows:] * added_w
        )


def put_spread(spread_ref, head):
    chunk = 8 * head
    shape = (spread_ref.shape[0], chunk)
    lane = lax.broadcasted_iota(jnp.int32, shape, 1) // head
    row = lax.broadcasted_iota(jnp.int32, shape, 0) % head
    for at in range(0, spread_ref.shape[1], chunk):
        hit = row == lane + at // head
        spread_ref[:, at : at + chunk] = jnp.where(hit, 1.0, 0.0).astype(jnp.bfloat16)


def fused_kernel(n, own_hbm, gain_hbm, bias_hbm, self_hbm, ro_hbm, *refs):
    weights, (w_out, state, mixed_ref, new_ref), refs = refs[:6], refs[6:10], refs[10:]
    spread_ref, gain_ref, bias_ref, self_ref, ro_ref, early, *refs = refs
    full_ref, next_ref, joined_ref, wo_ref, o_out, o_in, z_out, z_in, fin, fin_in, mine, *sems = refs
    load, g_send, g_recv, w_send, w_recv, o_send, o_recv, z_send, z_recv, f_send, f_recv = sems
    layers = state.shape[0]
    head = weights[0].shape[2]
    rows, columns = own_hbm.shape
    block = columns // 8
    deep = 8 * rows
    f32, bf16 = jnp.float32, jnp.bfloat16
    at = Place(n)

    def fetch(i, src, dst):
        copy = pltpu.make_async_copy(src, dst, early.at[i])
        copy.start()
        return copy

    own_load = fetch(0, own_hbm, full_ref.at[at.me])
    tables = [
        fetch(1, gain_hbm, gain_ref),
        fetch(2, bias_hbm, bias_ref),
        fetch(3, self_hbm, self_ref),
        fetch(4, ro_hbm, ro_ref),
    ]
    state_loads = []
    def load_bulk():
        for layer in range(layers):
            for i, w in enumerate(weights):
                copy = pltpu.make_async_copy(
                    w.at[layer, 0], joined_ref.at[layer, pl.ds(i * head, head)], load.at[layer, 0]
                )
                copy.start()
            copy = pltpu.make_async_copy(state.at[layer, 0], new_ref.at[layer, 0], load.at[layer, 1])
            copy.start()
            state_loads.append(copy)

    at.greet()
    own_cols = pl.ds(pl.multiple_of(at.i * block, block), block)
    own_slot = pl.ds(pl.multiple_of(at.i * head, head), head)
    own_weights = []

    def share_weights(layer):
        for to in at.others:
            cols = pl.ds(pl.multiple_of(to % 8 * block, block), block)
            copy = remote(
                w_out.at[layer, 0, :, cols],
                wo_ref.at[layer, own_slot],
                w_send.at[layer],
                w_recv.at[layer],
                to,
            )
            copy.start()
        copy = pltpu.make_async_copy(
            w_out.at[layer, 0, :, own_cols], wo_ref.at[layer, own_slot], load.at[layer, 2]
        )
        copy.start()
        own_weights.append(copy)

    def weights_here(layer):
        own_weights[layer].wait()
        slots = wo_ref.at[layer, pl.ds(0, 7 * head)]
        remote(slots, slots, w_send.at[layer], w_recv.at[layer], at.sib).wait()

    def mixer(layer, gather, reads, share_early, share_late):
        heads = []
        layer_state = new_ref.at[layer, 0]
        zero, a, b, c = [0] + at.near
        held = {}

        def here(k):
            return pl.ds(pl.multiple_of(at.plane(k) * deep, deep), deep)

        def projected(k):
            gather.finish(k)
            if not heads:
                if not layer:
                    for copy in tables:
                        copy.wait()
                whole = joined_ref.at[layer]
                pltpu.make_async_copy(whole, whole, load.at[layer, 0]).wait()
                heads.extend(own_head(t, layer, head) for t in (bias_ref, self_ref, ro_ref))
            held[k] = project(
                layer, functools.partial(reads, at.plane(k)), columns, gain_ref, joined_ref
            )

        def mixed_rows(k):
            if k == zero:
                state_loads[layer].wait()
            o, held[k] = read_state(held[k], heads, layer_state, here(k), spread_ref)
            packed = jnp.concatenate([o[: deep // 2], o[deep // 2 :]], axis=1).astype(bf16)
            o_out[layer, k] = packed
            o_in[layer, k, at.i] = packed
            for to in at.others:
                remote(
                    o_out.at[layer, k], o_in.at[layer, k, at.i], o_send.at[k], o_recv.at[k], to
                ).start()

        def update(k):
            write_state(held[k], layer_state, here(k), spread_ref)

        def emit(k):
            slots = o_in.at[layer, k, pl.ds(0, 7)]
            remote(slots, slots, o_send.at[k], o_recv.at[k], at.sib).wait()
            tops, bottoms = [], []
            for j in range(8):
                got = o_in[layer, k, j]
                tops.append(got[:, :head])
                bottoms.append(got[:, head:])
            left = jnp.concatenate(
                [jnp.concatenate(tops, axis=1), jnp.concatenate(bottoms, axis=1)], axis=0
            )
            part = jnp.dot(left, wo_ref[layer], preferred_element_type=f32)
            if k == zero:
                mine[...] = part
                return
            z_out[layer, k] = part.astype(bf16)
            remote(
                z_out.at[layer, k], z_in.at[layer, k], z_send.at[layer], z_recv.at[layer], at.zn(k)
            ).start()

        gather.middle_early()
        gather.adjacent()
        gather.sides(zero)
        gather.middle_late()
        gather.column(c)
        share_early()
        projected(zero)
        mixed_rows(zero)
        gather.sides(a)
        projected(a)
        gather.sides(b)
        mixed_rows(a)
        projected(b)
        gather.sides(c)
        mixed_rows(b)
        projected(c)
        mixed_rows(c)
        weights_here(layer)
        emit(a)
        emit(zero)
        emit(b)
        update(zero)
        update(a)
        emit(c)
        share_late()
        update(b)
        update(c)
        total = mine[...]
        slots = z_in.at[layer, pl.ds(1, at.planes - 1)]
        remote(slots, slots, z_send.at[layer], z_recv.at[layer], at.sib).wait()
        for k in at.near:
            total = total + z_in[layer, k].astype(f32)
        return total

    own_load.wait()
    first = Gather(at, full_ref.at[at.me], full_ref, g_send, g_recv)
    first.start()
    load_bulk()

    def first_reads(p, j):
        tiles = pl.ds(pl.multiple_of(p * 8, 8), 8)
        return full_ref[tiles, :, j * block : (j + 1) * block].reshape(deep, block)

    put_spread(spread_ref, head)
    total = mixer(
        0, first, first_reads, functools.partial(share_weights, 0), functools.partial(share_weights, 1)
    )
    mine_tiles = pl.ds(pl.multiple_of(at.z * 8, 8), 8)
    resid = full_ref[mine_tiles, :, own_cols].reshape(deep, block).astype(f32)
    piece = (resid + total).astype(bf16)
    first.drain()
    next_ref[at.me] = piece
    second = Gather(at, next_ref.at[at.me], next_ref, g_send, g_recv)
    second.start()
    nothing = lambda: None
    total = mixer(1, second, lambda p, j: next_ref[p * 8 + j], nothing, nothing)
    done = (next_ref[at.me].astype(f32) + total).astype(bf16)
    fin[...] = done.reshape(8, rows, block)
    fin_in[at.i] = fin[at.i]
    for to in at.others:
        remote(fin.at[to % 8], fin_in.at[at.i], f_send.at[0], f_recv.at[0], to).start()
    slots = fin_in.at[pl.ds(0, 7)]
    remote(slots, slots, f_send.at[0], f_recv.at[0], at.sib).wait()
    for j in range(8):
        mixed_ref[:, j * block : (j + 1) * block] = fin_in[j]
    second.drain()


WRITES = 4


def write_kernel(mixed_ref, state_ref, mixed_hbm, state_hbm, done):
    copies = [pltpu.make_async_copy(mixed_ref, mixed_hbm, done.at[0])]
    layers, _, rows, _ = state_ref.shape
    for layer in range(layers):
        for part in range(WRITES):
            here = pl.ds(part * (rows // WRITES), rows // WRITES)
            copies.append(
                pltpu.make_async_copy(
                    state_ref.at[layer, 0, here], state_hbm.at[layer, 0, here], done.at[len(copies)]
                )
            )
    for copy in copies:
        copy.start()
    for copy in copies:
        copy.wait()


def on_device_fast(n, *args):
    tokens, gain, wr, wk, wv, wd, wq, wg, bias, self_w, ro_gain, w_out, state = args
    weights = [jnp.swapaxes(w, 2, 3) for w in (wr, wk, wv, wd, wq, wg)]
    own = tokens[0]
    rows, columns = own.shape
    head = wr.shape[3]
    layers = state.shape[0]
    flat = state.shape[3]
    planes = n // 8
    block, deep = columns // 8, 8 * rows
    bf16, f32 = jnp.bfloat16, jnp.float32
    vmem, hbm = [pl.BlockSpec(memory_space=m) for m in (pltpu.VMEM, pltpu.HBM)]
    dma = pltpu.SemaphoreType.DMA
    stay = lambda a: pltpu.with_memory_space_constraint(a, pltpu.HBM)
    operands = [own, gain, bias, self_w, ro_gain, *weights, w_out, state]
    mixed, new_state = pl.pallas_call(
        functools.partial(fused_kernel, n),
        out_shape=(
            pltpu.VMEM(own.shape, own.dtype),
            pltpu.VMEM(state.shape, state.dtype),
        ),
        in_specs=[hbm] * len(operands),
        out_specs=(vmem, vmem),
        scratch_shapes=[
            pltpu.VMEM((2 * head, flat), bf16),
            *[pltpu.VMEM(t.shape, t.dtype) for t in (gain, bias, self_w, ro_gain)],
            dma((5,)),
            pltpu.VMEM((n, rows, columns), bf16),
            pltpu.VMEM((n, deep, block), bf16),
            pltpu.VMEM((layers, 6 * head, columns), bf16),
            pltpu.VMEM((layers, 8 * head, block), bf16),
            pltpu.VMEM((layers, planes, deep // 2, 2 * head), bf16),
            pltpu.VMEM((layers, planes, 8, deep // 2, 2 * head), bf16),
            pltpu.VMEM((layers, planes, deep, block), bf16),
            pltpu.VMEM((layers, planes, deep, block), bf16),
            pltpu.VMEM((8, rows, block), bf16),
            pltpu.VMEM((8, rows, block), bf16),
            pltpu.VMEM((deep, block), f32),
            dma((layers, 3)),
            dma((1,)),
            dma((5 * planes - 1,)),
            dma((layers,)),
            dma((layers,)),
            dma((planes,)),
            dma((planes,)),
            dma((layers,)),
            dma((layers,)),
            dma((1,)),
            dma((1,)),
        ],
        compiler_params=pltpu.CompilerParams(
            collective_id=0, has_side_effects=True, vmem_limit_bytes=40 << 20
        ),
        cost_estimate=pl.CostEstimate(flops=0, bytes_accessed=50 << 20, transcendentals=0),
    )(*[stay(o) for o in operands])
    held = [pltpu.with_memory_space_constraint(a, pltpu.VMEM) for a in (mixed, new_state)]
    mixed, new_state = pl.pallas_call(
        write_kernel,
        out_shape=[jax.ShapeDtypeStruct(a.shape, a.dtype) for a in held],
        in_specs=[vmem, vmem],
        out_specs=[hbm, hbm],
        scratch_shapes=[dma((1 + WRITES * layers,))],
        compiler_params=pltpu.CompilerParams(vmem_limit_bytes=1 << 20),
    )(*held)
    return mixed[None], new_state


def pick(n, *args):
    one_block = args[0].shape[2] == args[1].shape[1]
    tiles = args[0].shape[1] % 8 == 0 and args[0].shape[2] % 1024 == 0
    if one_block and tiles and n // 8 == 4 and 2 * args[2].shape[3] % 128 == 0:
        return on_device_fast(n, *args)
    return on_device(*args)


def solution(mesh):
    return jax.shard_map(
        functools.partial(pick, mesh.shape["tp"]),
        mesh=mesh,
        in_specs=(
            P("tp", None, None),
            P(),
            P(None, "tp", None, None),
            P(None, "tp", None, None),
            P(None, "tp", None, None),
            P(None, "tp", None, None),
            P(None, "tp", None, None),
            P(None, "tp", None, None),
            P(),
            P(),
            P(),
            P(None, "tp", None, None),
            P(None, "tp", None, None),
        ),
        out_specs=(P("tp", None, None), P(None, "tp", None, None)),
        check_vma=False,
    )
```

```python
import functools

import jax
import jax.numpy as jnp
from jax import lax
from jax.experimental import pallas as pl
from jax.experimental.pallas import tpu as pltpu
from jax.sharding import PartitionSpec as P

D = 4096


RMS_EPS = 1e-06
GROUP_EPS = 0.00064


def swapped(shard, axis, stride):
    return lax.ppermute(shard, axis, [(i, i ^ 1 << stride) for i in range(lax.axis_size(axis))])


def for_sending(shard):

    def short(part):
        return part.astype(jnp.bfloat16) if part.dtype == jnp.float32 else part

    return jax.tree.map(short, shard)


def recurrent_update(
    layer_state,
    receptance_vector,
    key_vector,
    value_vector,
    decay_logits,
    learning_rate_logits,
    gate_logits,
    decay_constant,
    self_term_scale,
    head_gain_slice,
):
    highest = lax.Precision.HIGHEST
    shrink = jnp.exp(-jnp.exp(-jax.nn.softplus(-(decay_constant + decay_logits)) - 0.5))
    rate = jax.nn.sigmoid(learning_rate_logits)
    normed = key_vector * lax.rsqrt(jnp.sum(key_vector * key_vector, -1, keepdims=True) + 1.0)
    removed = jnp.einsum("...ij,...j->...i", layer_state, normed, precision=highest)
    layer_state = (
        layer_state * shrink[..., None, :]
        - removed[..., :, None] * (normed * rate)[..., None, :]
        + value_vector[..., :, None] * (key_vector * rate)[..., None, :]
    )
    readout = jnp.einsum("...ij,...j->...i", layer_state, receptance_vector, precision=highest)
    center = jnp.mean(readout, -1, keepdims=True)
    spread = jnp.mean(jnp.square(readout - center), -1, keepdims=True)
    normed_output = (readout - center) * lax.rsqrt(spread + GROUP_EPS) * head_gain_slice
    self_term = (
        jnp.sum(receptance_vector * key_vector * self_term_scale, -1, keepdims=True) * value_vector
    )
    return (
        ((normed_output + self_term) * jax.nn.sigmoid(gate_logits)).astype(jnp.bfloat16),
        layer_state,
    )


def double_gather(piece, position, first_bit, count, mover):
    for offset in range(count):
        which_bit = first_bit + offset
        partner = mover(piece, which_bit)
        lower_self = position >> which_bit & 1 == 0
        piece = jnp.where(
            lower_self, jnp.concatenate([piece, partner], 0), jnp.concatenate([partner, piece], 0)
        )
    return piece


def halve_sum(members, position, first_bit, count, mover):
    for offset in reversed(range(count)):
        which_bit = first_bit + offset
        upper_self = position >> which_bit & 1 == 1
        sends = tuple(
            (
                jnp.where(
                    upper_self, member[: member.shape[0] // 2], member[member.shape[0] // 2 :]
                )
                for member in members
            )
        )
        keeps = tuple(
            (
                jnp.where(
                    upper_self, member[member.shape[0] // 2 :], member[: member.shape[0] // 2]
                )
                for member in members
            )
        )
        arrived = mover(sends, which_bit)
        members = tuple((kept + got for kept, got in zip(keeps, arrived)))
    return members


def on_device(
    tokens,
    block_norm_gain,
    receptance_weight,
    key_weight,
    value_weight,
    decay_weight,
    learning_rate_weight,
    gate_weight,
    decay_bias_fixed,
    self_token_weight,
    readout_norm_gain,
    output_weight,
    state,
):
    columns_dev = tokens.shape[2]
    row_blocks = D // columns_dev
    low_bits = row_blocks.bit_length() - 1
    head_count = lax.axis_size("tp") // row_blocks
    high_bits = head_count.bit_length() - 1
    position = lax.axis_index("tp")
    head_index = position // row_blocks
    row_block = position % row_blocks
    head_size = receptance_weight.shape[3]
    seq_tile = tokens.shape[1]
    move_rows = lambda payload, which_bit: swapped(payload, "tp", which_bit)
    move_proj = lambda payload, which_bit: swapped(payload, "tp", which_bit)
    move_outs = lambda payload, which_bit: jax.tree.map(
        lambda part, own: part.astype(own.dtype),
        swapped(for_sending(payload), "tp", which_bit),
        payload,
    )
    move_split = lambda payload, which_bit: jax.tree.map(
        lambda part, own: part.astype(own.dtype),
        swapped(for_sending(payload), "tp", which_bit),
        payload,
    )

    def mixer(columns, layer_index):
        gain_cols = lax.dynamic_slice_in_dim(
            block_norm_gain[layer_index], row_block * columns_dev, columns_dev
        )
        wide = columns.astype(jnp.float32)
        scaled = (wide * gain_cols).astype(jnp.bfloat16)
        squares = jnp.sum(wide * wide, axis=1)
        weights = jnp.concatenate(
            [
                receptance_weight[layer_index, 0],
                key_weight[layer_index, 0],
                value_weight[layer_index, 0],
                decay_weight[layer_index, 0],
                learning_rate_weight[layer_index, 0],
                gate_weight[layer_index, 0],
            ],
            axis=1,
        )
        partial_value = jnp.dot(scaled, weights, preferred_element_type=jnp.float32)
        summed, total_sq = halve_sum((partial_value, squares), position, 0, low_bits, move_proj)
        projected = summed * lax.rsqrt(total_sq / D + RMS_EPS)[:, None]
        output_pieces = jnp.split(projected, 6, axis=1)

        def head_columns(table):
            return lax.dynamic_slice_in_dim(table[layer_index], head_index * head_size, head_size)

        layer_state = state[layer_index, 0].reshape(-1, head_size, head_size)
        out_tile, layer_state = recurrent_update(
            layer_state,
            *output_pieces,
            head_columns(decay_bias_fixed),
            head_columns(self_token_weight),
            head_columns(readout_norm_gain)
        )
        out_all = double_gather(out_tile, position, 0, low_bits, move_outs)
        branch = jnp.dot(out_all, output_weight[layer_index, 0], preferred_element_type=jnp.float32)
        return (branch, layer_state.reshape(layer_state.shape[0], head_size * head_size))

    columns = double_gather(tokens[0], position, low_bits, high_bits, move_rows)
    first_branch, first_memory = mixer(columns, 0)
    (tile_sum,) = halve_sum((first_branch,), position, low_bits, high_bits, move_split)
    tile_one = (tokens[0].astype(jnp.float32) + tile_sum).astype(jnp.bfloat16)
    columns = double_gather(tile_one, position, low_bits, high_bits, move_rows)
    second_branch, second_memory = mixer(columns, 1)
    (tile_sum,) = halve_sum((second_branch,), position, low_bits, high_bits, move_split)
    resid_rows = lax.dynamic_slice_in_dim(columns, head_index * seq_tile, seq_tile, 0)
    mixed = (resid_rows.astype(jnp.float32) + tile_sum).astype(jnp.bfloat16)
    new_state = jnp.stack([first_memory, second_memory])[:, None]
    return (mixed[None], new_state)


class Place:
    def __init__(self, n):
        me = lax.axis_index("tp")
        self.n, self.planes = n, n // 8
        self.me = me
        self.i = me % 8
        self.c = me % 2
        self.x = (me // 2) % 2
        self.y = (me // 4) % 2
        self.z = me // 8
        self.sib = self.peer(0, 0, 1)
        self.xn = self.peer(0, 1, 0)
        self.yn = self.peer(1, 0, 0)
        flips = [(1, 1, 0), (1, 1, 1), (1, 0, 0), (1, 0, 1), (0, 1, 0), (0, 1, 1), (0, 0, 1)]
        self.others = [self.peer(*f) for f in flips]
        self.xyn = self.others[0]
        self.near = [1, 3, 2]

    def peer(self, dy, dx, dc):
        flip = lambda v, d: 1 - v if d else v
        return self.tile(self.z, flip(self.y, dy), flip(self.x, dx), flip(self.c, dc))

    def tile(self, p, y, x, c):
        return ((p * 2 + y) * 2 + x) * 2 + c

    def plane(self, k):
        low, high = self.z % 2, self.z // 2
        return 2 * (1 - high if k // 2 else high) + (1 - low if k % 2 else low)

    def zn(self, k):
        return self.plane(k) * 8 + self.i

    def greet(self):
        barrier = pltpu.get_barrier_semaphore()
        others = self.others + [self.zn(k) for k in self.near]
        for other in others:
            pl.semaphore_signal(
                barrier, inc=1, device_id=(other,), device_id_type=pl.DeviceIdType.MESH
            )
        pl.semaphore_wait(barrier, len(others))


def remote(src, dst, send, recv, to):
    return pltpu.make_async_remote_copy(
        src_ref=src,
        dst_ref=dst,
        send_sem=send,
        recv_sem=recv,
        device_id=(to,),
        device_id_type=pl.DeviceIdType.MESH,
    )


GATHER_SENDS = 3 + 4 + 1 + 2 * 4 + 6 + 3 * 3


class Gather:
    def __init__(self, at, own_ref, full_ref, send, recv):
        self.at, self.own, self.full = at, own_ref, full_ref
        self.send, self.recv = send, recv
        self.inner = at.z % 2 != at.z // 2

    def spot(self, k, i):
        return k * 4 + i

    def go(self, src, t, spot, *tos):
        for to in tos:
            remote(src, self.full.at[t], self.send.at[0], self.recv.at[spot], to).start()

    def arrived(self, spot, tiles=1):
        dst = self.full.at[pl.ds(0, tiles)]
        remote(dst, dst, self.send.at[0], self.recv.at[spot], self.at.sib).wait_recv()

    def cross(self, k, src, t):
        at = self.at
        tos = (at.xyn, at.xn, at.yn)
        for i in (0, 1, 2) if k else (1, 2, 0):
            self.go(src, t, self.spot(k, i), tos[i])
        self.to_sib(k, src, t)

    def to_sib(self, k, src, t):
        self.go(src, t, self.spot(k, 3), self.at.sib)

    def along(self, k):
        return 4 * self.at.planes + k - 1

    def start(self):
        at = self.at
        for k in (1, 3):
            self.go(self.own, at.me, self.along(k), at.zn(k))

        @pl.when(jnp.logical_not(self.inner))
        def _():
            self.go(self.own, at.me, self.along(2), at.zn(2))

        self.cross(0, self.own, at.me)

    def adjacent(self):
        t = self.at.zn(1)
        self.arrived(self.along(1))
        self.go(self.full.at[t], t, self.spot(1, 0), self.at.xyn)
        self.to_sib(1, self.full.at[t], t)

    def column(self, k):
        t = self.at.zn(k)
        self.arrived(self.along(k))
        self.cross(k, self.full.at[t], t)

    def middle_early(self):
        @pl.when(self.inner)
        def _():
            t = self.at.zn(3)
            self.arrived(self.along(3))
            self.go(self.full.at[t], t, self.along(2), self.at.zn(1))
            self.cross(3, self.full.at[t], t)

    def middle_late(self):
        @pl.when(jnp.logical_not(self.inner))
        def _():
            self.column(3)

    def sides(self, k):
        at = self.at
        p = at.plane(k)
        spots = ((1 - at.y, 1 - at.x), (at.y, 1 - at.x), (1 - at.y, at.x))
        for i in (1, 2, 0):
            y, x = spots[i]
            t = at.tile(p, y, x, at.c)
            self.arrived(self.spot(k, i))
            if not k and i:
                self.go(self.full.at[t], t, self.spot(1, i), at.zn(1))
            self.to_sib(k, self.full.at[t], t)

    def finish(self, k):
        self.arrived(self.spot(k, 3), 4)

    def drain(self):
        dst = self.full.at[pl.ds(0, GATHER_SENDS)]
        remote(dst, dst, self.send.at[0], self.recv.at[0], self.at.sib).wait_send()


def lanes(v, times):
    return jnp.concatenate([v] * times, axis=1)


def own_head(ref, layer, head):
    position = lax.axis_index("tp")
    start = pl.multiple_of(position // 2 * (2 * head), 2 * head)
    pair = ref[layer : layer + 1, pl.ds(start, 2 * head)]
    return jnp.where(position % 2 == 0, pair[:, :head], pair[:, head:])


def project(layer, read, columns, gain_ref, w_ref):
    chunk = columns // 8
    acc, squares = None, None
    for j in range(8):
        wide = read(j).astype(jnp.float32)
        cols = slice(j * chunk, (j + 1) * chunk)
        scaled = (wide * gain_ref[layer : layer + 1, cols]).astype(jnp.bfloat16)
        part = lax.dot_general(
            scaled,
            w_ref[layer, :, cols],
            (((1,), (1,)), ((), ())),
            preferred_element_type=jnp.float32,
        )
        square = wide * wide
        folded = square[:, :128]
        for lane in range(128, chunk, 128):
            folded = folded + square[:, lane : lane + 128]
        acc = part if acc is None else acc + part
        squares = folded if squares is None else squares + folded
    mean = jnp.sum(squares, axis=1, keepdims=True) / columns
    return acc * lax.rsqrt(mean + RMS_EPS)


def read_state(proj, heads, state_ref, at_rows, spread_ref):
    bias, self_w, ro_gain = heads
    head = bias.shape[1]
    rows = proj.shape[0]
    flat = state_ref.shape[1]
    chunk = 8 * head
    r, k, v, p, q, g = [proj[:, i * head : (i + 1) * head] for i in range(6)]
    decay = jnp.exp(-jax.nn.sigmoid(bias + p) * jnp.exp(jnp.float32(-0.5)))
    rate = jax.nn.sigmoid(q)
    kn = k * lax.rsqrt(jnp.sum(k * k, axis=1, keepdims=True) + 1.0)
    taken, added = kn * rate, k * rate
    kn_w, u_w = lanes(kn, chunk // head), lanes(decay * r, chunk // head)
    sums = jnp.zeros((2 * rows, head), jnp.float32)
    for at in range(0, flat, chunk):
        s = state_ref[at_rows, at : at + chunk]
        both = jnp.concatenate([s * kn_w, s * u_w], axis=0).astype(jnp.bfloat16)
        sums += lax.dot_general(
            both,
            spread_ref[:head, at : at + chunk],
            (((1,), (1,)), ((), ())),
            preferred_element_type=jnp.float32,
        )
    removed, read = sums[:rows], sums[rows:]
    read = (
        read
        - removed * jnp.sum(taken * r, axis=1, keepdims=True)
        + v * jnp.sum(added * r, axis=1, keepdims=True)
    )
    center = jnp.mean(read, axis=1, keepdims=True)
    off = read - center
    spread = jnp.mean(off * off, axis=1, keepdims=True)
    normed = off * lax.rsqrt(spread + GROUP_EPS) * ro_gain
    own_term = jnp.sum(r * k * self_w, axis=1, keepdims=True) * v
    o = (normed + own_term) * jax.nn.sigmoid(g)
    return o, (removed, v, decay, taken, added)


def write_state(parts, state_ref, at_rows, spread_ref):
    removed, v, decay, taken, added = parts
    rows, head = v.shape
    flat = state_ref.shape[1]
    chunk = 8 * head
    pair = jnp.concatenate([removed, v], axis=0)
    high = pair.astype(jnp.bfloat16)
    low = (pair - high.astype(jnp.float32)).astype(jnp.bfloat16)
    pair = jnp.concatenate([high, low], axis=1)
    decay_w, taken_w, added_w = [lanes(t, chunk // head) for t in (decay, taken, added)]
    for at in range(0, flat, chunk):
        wide = jnp.dot(pair, spread_ref[:, at : at + chunk], preferred_element_type=jnp.float32)
        state_ref[at_rows, at : at + chunk] = (
            state_ref[at_rows, at : at + chunk] * decay_w
            - wide[:rows] * taken_w
            + wide[rows:] * added_w
        )


def put_spread(spread_ref, head):
    chunk = 8 * head
    shape = (spread_ref.shape[0], chunk)
    lane = lax.broadcasted_iota(jnp.int32, shape, 1) // head
    row = lax.broadcasted_iota(jnp.int32, shape, 0) % head
    for at in range(0, spread_ref.shape[1], chunk):
        hit = row == lane + at // head
        spread_ref[:, at : at + chunk] = jnp.where(hit, 1.0, 0.0).astype(jnp.bfloat16)


def fused_kernel(n, own_hbm, gain_hbm, bias_hbm, self_hbm, ro_hbm, *refs):
    weights, (w_out, state, mixed_ref, new_ref), refs = refs[:6], refs[6:10], refs[10:]
    spread_ref, gain_ref, bias_ref, self_ref, ro_ref, early, *refs = refs
    full_ref, next_ref, joined_ref, wo_ref, o_out, o_in, z_out, z_in, fin, fin_in, mine, *sems = refs
    load, g_send, g_recv, w_send, w_recv, o_send, o_recv, z_send, z_recv, f_send, f_recv = sems
    layers = state.shape[0]
    head = weights[0].shape[2]
    rows, columns = own_hbm.shape
    block = columns // 8
    deep = 8 * rows
    f32, bf16 = jnp.float32, jnp.bfloat16
    at = Place(n)

    def fetch(i, src, dst):
        copy = pltpu.make_async_copy(src, dst, early.at[i])
        copy.start()
        return copy

    own_load = fetch(0, own_hbm, full_ref.at[at.me])
    tables = [
        fetch(1, gain_hbm, gain_ref),
        fetch(2, bias_hbm, bias_ref),
        fetch(3, self_hbm, self_ref),
        fetch(4, ro_hbm, ro_ref),
    ]
    state_loads = []
    def load_bulk():
        for layer in range(layers):
            for i, w in enumerate(weights):
                copy = pltpu.make_async_copy(
                    w.at[layer, 0], joined_ref.at[layer, pl.ds(i * head, head)], load.at[layer, 0]
                )
                copy.start()
            copy = pltpu.make_async_copy(state.at[layer, 0], new_ref.at[layer, 0], load.at[layer, 1])
            copy.start()
            state_loads.append(copy)

    at.greet()
    own_cols = pl.ds(pl.multiple_of(at.i * block, block), block)
    own_slot = pl.ds(pl.multiple_of(at.i * head, head), head)
    own_weights = []

    def share_weights(layer):
        for to in at.others:
            cols = pl.ds(pl.multiple_of(to % 8 * block, block), block)
            copy = remote(
                w_out.at[layer, 0, :, cols],
                wo_ref.at[layer, own_slot],
                w_send.at[layer],
                w_recv.at[layer],
                to,
            )
            copy.start()
        copy = pltpu.make_async_copy(
            w_out.at[layer, 0, :, own_cols], wo_ref.at[layer, own_slot], load.at[layer, 2]
        )
        copy.start()
        own_weights.append(copy)

    def weights_here(layer):
        own_weights[layer].wait()
        slots = wo_ref.at[layer, pl.ds(0, 7 * head)]
        remote(slots, slots, w_send.at[layer], w_recv.at[layer], at.sib).wait()

    def mixer(layer, gather, reads, share_early, share_late):
        heads = []
        layer_state = new_ref.at[layer, 0]
        zero, a, b, c = [0] + at.near
        held = {}

        def here(k):
            return pl.ds(pl.multiple_of(at.plane(k) * deep, deep), deep)

        def projected(k):
            gather.finish(k)
            if not heads:
                if not layer:
                    for copy in tables:
                        copy.wait()
                whole = joined_ref.at[layer]
                pltpu.make_async_copy(whole, whole, load.at[layer, 0]).wait()
                heads.extend(own_head(t, layer, head) for t in (bias_ref, self_ref, ro_ref))
            held[k] = project(
                layer, functools.partial(reads, at.plane(k)), columns, gain_ref, joined_ref
            )

        def mixed_rows(k):
            if k == zero:
                state_loads[layer].wait()
            o, held[k] = read_state(held[k], heads, layer_state, here(k), spread_ref)
            packed = jnp.concatenate([o[: deep // 2], o[deep // 2 :]], axis=1).astype(bf16)
            o_out[layer, k] = packed
            o_in[layer, k, at.i] = packed
            for to in at.others:
                remote(
                    o_out.at[layer, k], o_in.at[layer, k, at.i], o_send.at[k], o_recv.at[k], to
                ).start()

        def update(k):
            write_state(held[k], layer_state, here(k), spread_ref)

        def emit(k):
            slots = o_in.at[layer, k, pl.ds(0, 7)]
            remote(slots, slots, o_send.at[k], o_recv.at[k], at.sib).wait()
            tops, bottoms = [], []
            for j in range(8):
                got = o_in[layer, k, j]
                tops.append(got[:, :head])
                bottoms.append(got[:, head:])
            left = jnp.concatenate(
                [jnp.concatenate(tops, axis=1), jnp.concatenate(bottoms, axis=1)], axis=0
            )
            part = jnp.dot(left, wo_ref[layer], preferred_element_type=f32)
            if layer == layers - 1:
                fin[k] = part.astype(bf16).reshape(8, rows, block)
                if k == zero:
                    fin_in[k * 8 + at.i] = fin[k, at.i]
                for to in at.others if k == zero else [at.plane(k) * 8 + j for j in range(8)]:
                    remote(
                        fin.at[k, to % 8], fin_in.at[k * 8 + at.i], f_send.at[0], f_recv.at[0], to
                    ).start()
                return
            if k == zero:
                mine[...] = part
                return
            z_out[layer, k] = part.astype(bf16)
            remote(
                z_out.at[layer, k], z_in.at[layer, k], z_send.at[layer], z_recv.at[layer], at.zn(k)
            ).start()

        gather.middle_early()
        gather.adjacent()
        gather.sides(zero)
        gather.middle_late()
        gather.column(c)
        share_early()
        projected(zero)
        mixed_rows(zero)
        gather.sides(a)
        projected(a)
        gather.sides(b)
        mixed_rows(a)
        projected(b)
        gather.sides(c)
        mixed_rows(b)
        projected(c)
        mixed_rows(c)
        weights_here(layer)
        emit(a)
        emit(zero)
        emit(b)
        update(zero)
        update(a)
        emit(c)
        share_late()
        update(b)
        update(c)
        if layer == layers - 1:
            return None
        total = mine[...]
        slots = z_in.at[layer, pl.ds(1, at.planes - 1)]
        remote(slots, slots, z_send.at[layer], z_recv.at[layer], at.sib).wait()
        for k in at.near:
            total = total + z_in[layer, k].astype(f32)
        return total

    own_load.wait()
    first = Gather(at, full_ref.at[at.me], full_ref, g_send, g_recv)
    first.start()
    load_bulk()

    def first_reads(p, j):
        tiles = pl.ds(pl.multiple_of(p * 8, 8), 8)
        return full_ref[tiles, :, j * block : (j + 1) * block].reshape(deep, block)

    put_spread(spread_ref, head)
    total = mixer(
        0, first, first_reads, functools.partial(share_weights, 0), functools.partial(share_weights, 1)
    )
    mine_tiles = pl.ds(pl.multiple_of(at.z * 8, 8), 8)
    resid = full_ref[mine_tiles, :, own_cols].reshape(deep, block).astype(f32)
    piece = (resid + total).astype(bf16)
    first.drain()
    next_ref[at.me] = piece.reshape(8, rows, block)
    second = Gather(at, next_ref.at[at.me], next_ref, g_send, g_recv)
    second.start()
    nothing = lambda: None
    second_reads = lambda p, j: next_ref[p * 8 + j].reshape(deep, block)
    mixer(1, second, second_reads, nothing, nothing)
    slots = fin_in.at[pl.ds(0, n - 1)]
    remote(slots, slots, f_send.at[0], f_recv.at[0], at.sib).wait()
    for j in range(8):
        tile = next_ref[at.z * 8 + j, at.i].astype(f32)
        for k in range(at.planes):
            tile = tile + fin_in[k * 8 + j].astype(f32)
        mixed_ref[:, j * block : (j + 1) * block] = tile.astype(bf16)
    second.drain()


WRITES = 4


def write_kernel(mixed_ref, state_ref, mixed_hbm, state_hbm, done):
    copies = [pltpu.make_async_copy(mixed_ref, mixed_hbm, done.at[0])]
    layers, _, rows, _ = state_ref.shape
    for layer in range(layers):
        for part in range(WRITES):
            here = pl.ds(part * (rows // WRITES), rows // WRITES)
            copies.append(
                pltpu.make_async_copy(
                    state_ref.at[layer, 0, here], state_hbm.at[layer, 0, here], done.at[len(copies)]
                )
            )
    for copy in copies:
        copy.start()
    for copy in copies:
        copy.wait()


def on_device_fast(n, *args):
    tokens, gain, wr, wk, wv, wd, wq, wg, bias, self_w, ro_gain, w_out, state = args
    weights = [jnp.swapaxes(w, 2, 3) for w in (wr, wk, wv, wd, wq, wg)]
    own = tokens[0]
    rows, columns = own.shape
    head = wr.shape[3]
    layers = state.shape[0]
    flat = state.shape[3]
    planes = n // 8
    block, deep = columns // 8, 8 * rows
    bf16, f32 = jnp.bfloat16, jnp.float32
    vmem, hbm = [pl.BlockSpec(memory_space=m) for m in (pltpu.VMEM, pltpu.HBM)]
    dma = pltpu.SemaphoreType.DMA
    stay = lambda a: pltpu.with_memory_space_constraint(a, pltpu.HBM)
    operands = [own, gain, bias, self_w, ro_gain, *weights, w_out, state]
    mixed, new_state = pl.pallas_call(
        functools.partial(fused_kernel, n),
        out_shape=(
            pltpu.VMEM(own.shape, own.dtype),
            pltpu.VMEM(state.shape, state.dtype),
        ),
        in_specs=[hbm] * len(operands),
        out_specs=(vmem, vmem),
        scratch_shapes=[
            pltpu.VMEM((2 * head, flat), bf16),
            *[pltpu.VMEM(t.shape, t.dtype) for t in (gain, bias, self_w, ro_gain)],
            dma((5,)),
            pltpu.VMEM((n, rows, columns), bf16),
            pltpu.VMEM((n, 8, rows, block), bf16),
            pltpu.VMEM((layers, 6 * head, columns), bf16),
            pltpu.VMEM((layers, 8 * head, block), bf16),
            pltpu.VMEM((layers, planes, deep // 2, 2 * head), bf16),
            pltpu.VMEM((layers, planes, 8, deep // 2, 2 * head), bf16),
            pltpu.VMEM((layers, planes, deep, block), bf16),
            pltpu.VMEM((layers, planes, deep, block), bf16),
            pltpu.VMEM((planes, 8, rows, block), bf16),
            pltpu.VMEM((n, rows, block), bf16),
            pltpu.VMEM((deep, block), f32),
            dma((layers, 3)),
            dma((1,)),
            dma((5 * planes - 1,)),
            dma((layers,)),
            dma((layers,)),
            dma((planes,)),
            dma((planes,)),
            dma((layers,)),
            dma((layers,)),
            dma((1,)),
            dma((1,)),
        ],
        compiler_params=pltpu.CompilerParams(
            collective_id=0, has_side_effects=True, vmem_limit_bytes=40 << 20
        ),
        cost_estimate=pl.CostEstimate(flops=0, bytes_accessed=50 << 20, transcendentals=0),
    )(*[stay(o) for o in operands])
    held = [pltpu.with_memory_space_constraint(a, pltpu.VMEM) for a in (mixed, new_state)]
    mixed, new_state = pl.pallas_call(
        write_kernel,
        out_shape=[jax.ShapeDtypeStruct(a.shape, a.dtype) for a in held],
        in_specs=[vmem, vmem],
        out_specs=[hbm, hbm],
        scratch_shapes=[dma((1 + WRITES * layers,))],
        compiler_params=pltpu.CompilerParams(vmem_limit_bytes=1 << 20),
    )(*held)
    return mixed[None], new_state


def pick(n, *args):
    one_block = args[0].shape[2] == args[1].shape[1]
    tiles = args[0].shape[1] % 8 == 0 and args[0].shape[2] % 1024 == 0
    if one_block and tiles and n // 8 == 4 and 2 * args[2].shape[3] % 128 == 0:
        return on_device_fast(n, *args)
    return on_device(*args)


def solution(mesh):
    return jax.shard_map(
        functools.partial(pick, mesh.shape["tp"]),
        mesh=mesh,
        in_specs=(
            P("tp", None, None),
            P(),
            P(None, "tp", None, None),
            P(None, "tp", None, None),
            P(None, "tp", None, None),
            P(None, "tp", None, None),
            P(None, "tp", None, None),
            P(None, "tp", None, None),
            P(),
            P(),
            P(),
            P(None, "tp", None, None),
            P(None, "tp", None, None),
        ),
        out_specs=(P("tp", None, None), P(None, "tp", None, None)),
        check_vma=False,
    )
```

```python
import functools

import jax
import jax.numpy as jnp
from jax import lax
from jax.experimental import pallas as pl
from jax.experimental.pallas import tpu as pltpu
from jax.sharding import PartitionSpec as P

D = 4096


RMS_EPS = 1e-06
GROUP_EPS = 0.00064


def swapped(shard, axis, stride):
    return lax.ppermute(shard, axis, [(i, i ^ 1 << stride) for i in range(lax.axis_size(axis))])


def for_sending(shard):

    def short(part):
        return part.astype(jnp.bfloat16) if part.dtype == jnp.float32 else part

    return jax.tree.map(short, shard)


def recurrent_update(
    layer_state,
    receptance_vector,
    key_vector,
    value_vector,
    decay_logits,
    learning_rate_logits,
    gate_logits,
    decay_constant,
    self_term_scale,
    head_gain_slice,
):
    highest = lax.Precision.HIGHEST
    shrink = jnp.exp(-jnp.exp(-jax.nn.softplus(-(decay_constant + decay_logits)) - 0.5))
    rate = jax.nn.sigmoid(learning_rate_logits)
    normed = key_vector * lax.rsqrt(jnp.sum(key_vector * key_vector, -1, keepdims=True) + 1.0)
    removed = jnp.einsum("...ij,...j->...i", layer_state, normed, precision=highest)
    layer_state = (
        layer_state * shrink[..., None, :]
        - removed[..., :, None] * (normed * rate)[..., None, :]
        + value_vector[..., :, None] * (key_vector * rate)[..., None, :]
    )
    readout = jnp.einsum("...ij,...j->...i", layer_state, receptance_vector, precision=highest)
    center = jnp.mean(readout, -1, keepdims=True)
    spread = jnp.mean(jnp.square(readout - center), -1, keepdims=True)
    normed_output = (readout - center) * lax.rsqrt(spread + GROUP_EPS) * head_gain_slice
    self_term = (
        jnp.sum(receptance_vector * key_vector * self_term_scale, -1, keepdims=True) * value_vector
    )
    return (
        ((normed_output + self_term) * jax.nn.sigmoid(gate_logits)).astype(jnp.bfloat16),
        layer_state,
    )


def double_gather(piece, position, first_bit, count, mover):
    for offset in range(count):
        which_bit = first_bit + offset
        partner = mover(piece, which_bit)
        lower_self = position >> which_bit & 1 == 0
        piece = jnp.where(
            lower_self, jnp.concatenate([piece, partner], 0), jnp.concatenate([partner, piece], 0)
        )
    return piece


def halve_sum(members, position, first_bit, count, mover):
    for offset in reversed(range(count)):
        which_bit = first_bit + offset
        upper_self = position >> which_bit & 1 == 1
        sends = tuple(
            (
                jnp.where(
                    upper_self, member[: member.shape[0] // 2], member[member.shape[0] // 2 :]
                )
                for member in members
            )
        )
        keeps = tuple(
            (
                jnp.where(
                    upper_self, member[member.shape[0] // 2 :], member[: member.shape[0] // 2]
                )
                for member in members
            )
        )
        arrived = mover(sends, which_bit)
        members = tuple((kept + got for kept, got in zip(keeps, arrived)))
    return members


def on_device(
    tokens,
    block_norm_gain,
    receptance_weight,
    key_weight,
    value_weight,
    decay_weight,
    learning_rate_weight,
    gate_weight,
    decay_bias_fixed,
    self_token_weight,
    readout_norm_gain,
    output_weight,
    state,
):
    columns_dev = tokens.shape[2]
    row_blocks = D // columns_dev
    low_bits = row_blocks.bit_length() - 1
    head_count = lax.axis_size("tp") // row_blocks
    high_bits = head_count.bit_length() - 1
    position = lax.axis_index("tp")
    head_index = position // row_blocks
    row_block = position % row_blocks
    head_size = receptance_weight.shape[3]
    seq_tile = tokens.shape[1]
    move_rows = lambda payload, which_bit: swapped(payload, "tp", which_bit)
    move_proj = lambda payload, which_bit: swapped(payload, "tp", which_bit)
    move_outs = lambda payload, which_bit: jax.tree.map(
        lambda part, own: part.astype(own.dtype),
        swapped(for_sending(payload), "tp", which_bit),
        payload,
    )
    move_split = lambda payload, which_bit: jax.tree.map(
        lambda part, own: part.astype(own.dtype),
        swapped(for_sending(payload), "tp", which_bit),
        payload,
    )

    def mixer(columns, layer_index):
        gain_cols = lax.dynamic_slice_in_dim(
            block_norm_gain[layer_index], row_block * columns_dev, columns_dev
        )
        wide = columns.astype(jnp.float32)
        scaled = (wide * gain_cols).astype(jnp.bfloat16)
        squares = jnp.sum(wide * wide, axis=1)
        weights = jnp.concatenate(
            [
                receptance_weight[layer_index, 0],
                key_weight[layer_index, 0],
                value_weight[layer_index, 0],
                decay_weight[layer_index, 0],
                learning_rate_weight[layer_index, 0],
                gate_weight[layer_index, 0],
            ],
            axis=1,
        )
        partial_value = jnp.dot(scaled, weights, preferred_element_type=jnp.float32)
        summed, total_sq = halve_sum((partial_value, squares), position, 0, low_bits, move_proj)
        projected = summed * lax.rsqrt(total_sq / D + RMS_EPS)[:, None]
        output_pieces = jnp.split(projected, 6, axis=1)

        def head_columns(table):
            return lax.dynamic_slice_in_dim(table[layer_index], head_index * head_size, head_size)

        layer_state = state[layer_index, 0].reshape(-1, head_size, head_size)
        out_tile, layer_state = recurrent_update(
            layer_state,
            *output_pieces,
            head_columns(decay_bias_fixed),
            head_columns(self_token_weight),
            head_columns(readout_norm_gain)
        )
        out_all = double_gather(out_tile, position, 0, low_bits, move_outs)
        branch = jnp.dot(out_all, output_weight[layer_index, 0], preferred_element_type=jnp.float32)
        return (branch, layer_state.reshape(layer_state.shape[0], head_size * head_size))

    columns = double_gather(tokens[0], position, low_bits, high_bits, move_rows)
    first_branch, first_memory = mixer(columns, 0)
    (tile_sum,) = halve_sum((first_branch,), position, low_bits, high_bits, move_split)
    tile_one = (tokens[0].astype(jnp.float32) + tile_sum).astype(jnp.bfloat16)
    columns = double_gather(tile_one, position, low_bits, high_bits, move_rows)
    second_branch, second_memory = mixer(columns, 1)
    (tile_sum,) = halve_sum((second_branch,), position, low_bits, high_bits, move_split)
    resid_rows = lax.dynamic_slice_in_dim(columns, head_index * seq_tile, seq_tile, 0)
    mixed = (resid_rows.astype(jnp.float32) + tile_sum).astype(jnp.bfloat16)
    new_state = jnp.stack([first_memory, second_memory])[:, None]
    return (mixed[None], new_state)


class Place:
    def __init__(self, n):
        me = lax.axis_index("tp")
        self.n, self.planes = n, n // 8
        self.me = me
        self.i = me % 8
        self.c = me % 2
        self.x = (me // 2) % 2
        self.y = (me // 4) % 2
        self.z = me // 8
        self.sib = self.peer(0, 0, 1)
        self.xn = self.peer(0, 1, 0)
        self.yn = self.peer(1, 0, 0)
        flips = [(1, 1, 0), (1, 1, 1), (1, 0, 0), (1, 0, 1), (0, 1, 0), (0, 1, 1), (0, 0, 1)]
        self.others = [self.peer(*f) for f in flips]
        self.xyn = self.others[0]
        self.near = [1, 3, 2]

    def peer(self, dy, dx, dc):
        flip = lambda v, d: 1 - v if d else v
        return self.tile(self.z, flip(self.y, dy), flip(self.x, dx), flip(self.c, dc))

    def tile(self, p, y, x, c):
        return ((p * 2 + y) * 2 + x) * 2 + c

    def plane(self, k):
        low, high = self.z % 2, self.z // 2
        return 2 * (1 - high if k // 2 else high) + (1 - low if k % 2 else low)

    def zn(self, k):
        return self.plane(k) * 8 + self.i

    def greet(self):
        barrier = pltpu.get_barrier_semaphore()
        others = self.others + [self.zn(k) for k in self.near]
        for other in others:
            pl.semaphore_signal(
                barrier, inc=1, device_id=(other,), device_id_type=pl.DeviceIdType.MESH
            )
        pl.semaphore_wait(barrier, len(others))


def remote(src, dst, send, recv, to):
    return pltpu.make_async_remote_copy(
        src_ref=src,
        dst_ref=dst,
        send_sem=send,
        recv_sem=recv,
        device_id=(to,),
        device_id_type=pl.DeviceIdType.MESH,
    )


GATHER_SENDS = 3 + 4 + 1 + 2 * 4 + 6 + 3 * 3


class Gather:
    def __init__(self, at, own_ref, full_ref, send, recv):
        self.at, self.own, self.full = at, own_ref, full_ref
        self.send, self.recv = send, recv
        self.inner = at.z % 2 != at.z // 2

    def spot(self, k, i):
        return k * 4 + i

    def go(self, src, t, spot, *tos):
        for to in tos:
            remote(src, self.full.at[t], self.send.at[0], self.recv.at[spot], to).start()

    def arrived(self, spot, tiles=1):
        dst = self.full.at[pl.ds(0, tiles)]
        remote(dst, dst, self.send.at[0], self.recv.at[spot], self.at.sib).wait_recv()

    def cross(self, k, src, t):
        at = self.at
        tos = (at.xyn, at.xn, at.yn)
        for i in (0, 1, 2) if k else (1, 2, 0):
            self.go(src, t, self.spot(k, i), tos[i])
        self.to_sib(k, src, t)

    def to_sib(self, k, src, t):
        self.go(src, t, self.spot(k, 3), self.at.sib)

    def along(self, k):
        return 4 * self.at.planes + k - 1

    def start(self):
        at = self.at
        for k in (1, 3):
            self.go(self.own, at.me, self.along(k), at.zn(k))

        @pl.when(jnp.logical_not(self.inner))
        def _():
            self.go(self.own, at.me, self.along(2), at.zn(2))

        self.cross(0, self.own, at.me)

    def adjacent(self):
        t = self.at.zn(1)
        self.arrived(self.along(1))
        self.go(self.full.at[t], t, self.spot(1, 0), self.at.xyn)
        self.to_sib(1, self.full.at[t], t)

    def column(self, k):
        t = self.at.zn(k)
        self.arrived(self.along(k))
        self.cross(k, self.full.at[t], t)

    def middle_early(self):
        @pl.when(self.inner)
        def _():
            t = self.at.zn(3)
            self.arrived(self.along(3))
            self.go(self.full.at[t], t, self.along(2), self.at.zn(1))
            self.cross(3, self.full.at[t], t)

    def middle_late(self):
        @pl.when(jnp.logical_not(self.inner))
        def _():
            self.column(3)

    def sides(self, k, which=(1, 2, 0)):
        at = self.at
        p = at.plane(k)
        spots = ((1 - at.y, 1 - at.x), (at.y, 1 - at.x), (1 - at.y, at.x))
        for i in which:
            y, x = spots[i]
            t = at.tile(p, y, x, at.c)
            self.arrived(self.spot(k, i))
            if not k and i:
                self.go(self.full.at[t], t, self.spot(1, i), at.zn(1))
            self.to_sib(k, self.full.at[t], t)

    def finish(self, k):
        self.arrived(self.spot(k, 3), 4)

    def drain(self):
        dst = self.full.at[pl.ds(0, GATHER_SENDS)]
        remote(dst, dst, self.send.at[0], self.recv.at[0], self.at.sib).wait_send()


def lanes(v, times):
    return jnp.concatenate([v] * times, axis=1)


def own_head(ref, layer, head):
    position = lax.axis_index("tp")
    start = pl.multiple_of(position // 2 * (2 * head), 2 * head)
    pair = ref[layer : layer + 1, pl.ds(start, 2 * head)]
    return jnp.where(position % 2 == 0, pair[:, :head], pair[:, head:])


def project(layer, read, columns, gain_ref, w_ref):
    chunk = columns // 8
    acc, squares = None, None
    for j in range(8):
        wide = read(j).astype(jnp.float32)
        cols = slice(j * chunk, (j + 1) * chunk)
        scaled = (wide * gain_ref[layer : layer + 1, cols]).astype(jnp.bfloat16)
        part = lax.dot_general(
            scaled,
            w_ref[layer, :, cols],
            (((1,), (1,)), ((), ())),
            preferred_element_type=jnp.float32,
        )
        square = wide * wide
        folded = square[:, :128]
        for lane in range(128, chunk, 128):
            folded = folded + square[:, lane : lane + 128]
        acc = part if acc is None else acc + part
        squares = folded if squares is None else squares + folded
    mean = jnp.sum(squares, axis=1, keepdims=True) / columns
    return acc * lax.rsqrt(mean + RMS_EPS)


def read_state(proj, heads, state_ref, at_rows, spread_ref):
    take = lambda cols: [state_ref[here, cols] for here in at_rows]
    bias, self_w, ro_gain = heads
    head = bias.shape[1]
    rows = proj.shape[0]
    flat = state_ref.shape[1]
    chunk = 8 * head
    r, k, v, p, q, g = [proj[:, i * head : (i + 1) * head] for i in range(6)]
    decay = jnp.exp(-jax.nn.sigmoid(bias + p) * jnp.exp(jnp.float32(-0.5)))
    rate = jax.nn.sigmoid(q)
    kn = k * lax.rsqrt(jnp.sum(k * k, axis=1, keepdims=True) + 1.0)
    taken, added = kn * rate, k * rate
    kn_w, u_w = lanes(kn, chunk // head), lanes(decay * r, chunk // head)
    sums = jnp.zeros((2 * rows, head), jnp.float32)
    for at in range(0, flat, chunk):
        s = jnp.concatenate(take(slice(at, at + chunk)), axis=0)
        both = jnp.concatenate([s * kn_w, s * u_w], axis=0).astype(jnp.bfloat16)
        sums += lax.dot_general(
            both,
            spread_ref[:head, at : at + chunk],
            (((1,), (1,)), ((), ())),
            preferred_element_type=jnp.float32,
        )
    removed, read = sums[:rows], sums[rows:]
    read = (
        read
        - removed * jnp.sum(taken * r, axis=1, keepdims=True)
        + v * jnp.sum(added * r, axis=1, keepdims=True)
    )
    center = jnp.mean(read, axis=1, keepdims=True)
    off = read - center
    spread = jnp.mean(off * off, axis=1, keepdims=True)
    normed = off * lax.rsqrt(spread + GROUP_EPS) * ro_gain
    own_term = jnp.sum(r * k * self_w, axis=1, keepdims=True) * v
    o = (normed + own_term) * jax.nn.sigmoid(g)
    return o, (removed, v, decay, taken, added)


def write_state(parts, state_ref, at_rows, spread_ref):
    removed, v, decay, taken, added = parts
    rows, head = v.shape
    flat = state_ref.shape[1]
    chunk = 8 * head
    pair = jnp.concatenate([removed, v], axis=0)
    high = pair.astype(jnp.bfloat16)
    low = (pair - high.astype(jnp.float32)).astype(jnp.bfloat16)
    pair = jnp.concatenate([high, low], axis=1)
    decay_w, taken_w, added_w = [lanes(t, chunk // head) for t in (decay, taken, added)]
    for at in range(0, flat, chunk):
        wide = jnp.dot(pair, spread_ref[:, at : at + chunk], preferred_element_type=jnp.float32)
        state_ref[at_rows, at : at + chunk] = (
            state_ref[at_rows, at : at + chunk] * decay_w
            - wide[:rows] * taken_w
            + wide[rows:] * added_w
        )


def put_spread(spread_ref, head):
    chunk = 8 * head
    shape = (spread_ref.shape[0], chunk)
    lane = lax.broadcasted_iota(jnp.int32, shape, 1) // head
    row = lax.broadcasted_iota(jnp.int32, shape, 0) % head
    for at in range(0, spread_ref.shape[1], chunk):
        hit = row == lane + at // head
        spread_ref[:, at : at + chunk] = jnp.where(hit, 1.0, 0.0).astype(jnp.bfloat16)


def fused_kernel(n, own_hbm, gain_hbm, bias_hbm, self_hbm, ro_hbm, *refs):
    weights, (w_out, state, mixed_ref, new_ref), refs = refs[:6], refs[6:10], refs[10:]
    spread_ref, gain_ref, bias_ref, self_ref, ro_ref, early, *refs = refs
    full_ref, next_ref, joined_ref, wo_ref, o_out, o_in, z_out, z_in, fin, fin_in, mine, *sems = refs
    load, g_send, g_recv, w_send, w_recv, o_send, o_recv, z_send, z_recv, f_send, f_recv = sems
    layers = state.shape[0]
    head = weights[0].shape[2]
    rows, columns = own_hbm.shape
    block = columns // 8
    deep = 8 * rows
    f32, bf16 = jnp.float32, jnp.bfloat16
    at = Place(n)

    def fetch(i, src, dst):
        copy = pltpu.make_async_copy(src, dst, early.at[i])
        copy.start()
        return copy

    own_load = fetch(0, own_hbm, full_ref.at[at.me])
    tables = [
        fetch(1, gain_hbm, gain_ref),
        fetch(2, bias_hbm, bias_ref),
        fetch(3, self_hbm, self_ref),
        fetch(4, ro_hbm, ro_ref),
    ]
    state_loads = []
    def load_bulk():
        for layer in range(layers):
            for i, w in enumerate(weights):
                copy = pltpu.make_async_copy(
                    w.at[layer, 0], joined_ref.at[layer, pl.ds(i * head, head)], load.at[layer, 0]
                )
                copy.start()
            copy = pltpu.make_async_copy(state.at[layer, 0], new_ref.at[layer, 0], load.at[layer, 1])
            copy.start()
            state_loads.append(copy)

    at.greet()
    own_cols = pl.ds(pl.multiple_of(at.i * block, block), block)
    own_slot = pl.ds(pl.multiple_of(at.i * head, head), head)
    own_weights = []

    def share_weights(layer):
        for to in at.others:
            cols = pl.ds(pl.multiple_of(to % 8 * block, block), block)
            copy = remote(
                w_out.at[layer, 0, :, cols],
                wo_ref.at[layer, own_slot],
                w_send.at[layer],
                w_recv.at[layer],
                to,
            )
            copy.start()
        copy = pltpu.make_async_copy(
            w_out.at[layer, 0, :, own_cols], wo_ref.at[layer, own_slot], load.at[layer, 2]
        )
        copy.start()
        own_weights.append(copy)

    def weights_here(layer):
        own_weights[layer].wait()
        slots = wo_ref.at[layer, pl.ds(0, 7 * head)]
        remote(slots, slots, w_send.at[layer], w_recv.at[layer], at.sib).wait()

    def mixer(layer, gather, reads, share_early, share_late):
        heads = []
        layer_state = new_ref.at[layer, 0]
        zero, a, b, c = [0] + at.near
        held = {}

        def here(k):
            return pl.ds(pl.multiple_of(at.plane(k) * deep, deep), deep)

        def projected(*ks):
            for k in ks:
                gather.finish(k)
            if not heads:
                if not layer:
                    for copy in tables:
                        copy.wait()
                whole = joined_ref.at[layer]
                pltpu.make_async_copy(whole, whole, load.at[layer, 0]).wait()
                heads.extend(own_head(t, layer, head) for t in (bias_ref, self_ref, ro_ref))
            read = lambda j: jnp.concatenate([reads(at.plane(k), j) for k in ks], axis=0)
            held[ks] = project(layer, read, columns, gain_ref, joined_ref)

        def mixed_rows(*ks):
            if zero in ks:
                state_loads[layer].wait()
            rows_of = [here(k) for k in ks]
            o, parts = read_state(held[ks], heads, layer_state, rows_of, spread_ref)
            for m, k in enumerate(ks):
                cut = lambda t: t[m * deep : (m + 1) * deep]
                held[k] = [cut(t) for t in parts]
                top, bottom = cut(o)[: deep // 2], cut(o)[deep // 2 :]
                packed = jnp.concatenate([top, bottom], axis=1).astype(bf16)
                o_out[layer, k] = packed
                o_in[layer, k, at.i] = packed
                for to in at.others:
                    remote(
                        o_out.at[layer, k], o_in.at[layer, k, at.i], o_send.at[k], o_recv.at[k], to
                    ).start()

        def update(k):
            write_state(held[k], layer_state, here(k), spread_ref)

        def emit(k):
            slots = o_in.at[layer, k, pl.ds(0, 7)]
            remote(slots, slots, o_send.at[k], o_recv.at[k], at.sib).wait()
            tops, bottoms = [], []
            for j in range(8):
                got = o_in[layer, k, j]
                tops.append(got[:, :head])
                bottoms.append(got[:, head:])
            left = jnp.concatenate(
                [jnp.concatenate(tops, axis=1), jnp.concatenate(bottoms, axis=1)], axis=0
            )
            part = jnp.dot(left, wo_ref[layer], preferred_element_type=f32)
            if layer == layers - 1:
                fin[k] = part.astype(bf16).reshape(8, rows, block)
                if k == zero:
                    fin_in[k * 8 + at.i] = fin[k, at.i]
                for to in at.others if k == zero else [at.plane(k) * 8 + j for j in range(8)]:
                    remote(
                        fin.at[k, to % 8], fin_in.at[k * 8 + at.i], f_send.at[0], f_recv.at[0], to
                    ).start()
                return
            if k == zero:
                mine[...] = part
                return
            z_out[layer, k] = part.astype(bf16)
            remote(
                z_out.at[layer, k], z_in.at[layer, k], z_send.at[layer], z_recv.at[layer], at.zn(k)
            ).start()

        gather.middle_early()
        gather.adjacent()
        gather.sides(zero, (1, 2))
        gather.middle_late()
        gather.sides(zero, (0,))
        gather.column(c)
        projected(zero)
        mixed_rows(zero)
        gather.sides(a)
        gather.sides(b)
        share_early()
        projected(a, b)
        gather.sides(c)
        mixed_rows(a, b)
        projected(c)
        mixed_rows(c)
        weights_here(layer)
        emit(b)
        emit(a)
        emit(zero)
        update(zero)
        update(a)
        emit(c)
        share_late()
        update(b)
        update(c)
        if layer == layers - 1:
            return None
        total = mine[...]
        slots = z_in.at[layer, pl.ds(1, at.planes - 1)]
        remote(slots, slots, z_send.at[layer], z_recv.at[layer], at.sib).wait()
        for k in at.near:
            total = total + z_in[layer, k].astype(f32)
        return total

    own_load.wait()
    first = Gather(at, full_ref.at[at.me], full_ref, g_send, g_recv)
    first.start()
    load_bulk()

    def first_reads(p, j):
        tiles = pl.ds(pl.multiple_of(p * 8, 8), 8)
        return full_ref[tiles, :, j * block : (j + 1) * block].reshape(deep, block)

    put_spread(spread_ref, head)
    total = mixer(
        0, first, first_reads, functools.partial(share_weights, 0), functools.partial(share_weights, 1)
    )
    mine_tiles = pl.ds(pl.multiple_of(at.z * 8, 8), 8)
    resid = full_ref[mine_tiles, :, own_cols].reshape(deep, block).astype(f32)
    piece = (resid + total).astype(bf16)
    first.drain()
    next_ref[at.me] = piece.reshape(8, rows, block)
    second = Gather(at, next_ref.at[at.me], next_ref, g_send, g_recv)
    second.start()
    nothing = lambda: None
    second_reads = lambda p, j: next_ref[p * 8 + j].reshape(deep, block)
    mixer(1, second, second_reads, nothing, nothing)
    slots = fin_in.at[pl.ds(0, n - 1)]
    remote(slots, slots, f_send.at[0], f_recv.at[0], at.sib).wait()
    for j in range(8):
        tile = next_ref[at.z * 8 + j, at.i].astype(f32)
        for k in range(at.planes):
            tile = tile + fin_in[k * 8 + j].astype(f32)
        mixed_ref[:, j * block : (j + 1) * block] = tile.astype(bf16)
    second.drain()


WRITES = 4


def write_kernel(mixed_ref, state_ref, mixed_hbm, state_hbm, done):
    copies = [pltpu.make_async_copy(mixed_ref, mixed_hbm, done.at[0])]
    layers, _, rows, _ = state_ref.shape
    for layer in range(layers):
        for part in range(WRITES):
            here = pl.ds(part * (rows // WRITES), rows // WRITES)
            copies.append(
                pltpu.make_async_copy(
                    state_ref.at[layer, 0, here], state_hbm.at[layer, 0, here], done.at[len(copies)]
                )
            )
    for copy in copies:
        copy.start()
    for copy in copies:
        copy.wait()


def on_device_fast(n, *args):
    tokens, gain, wr, wk, wv, wd, wq, wg, bias, self_w, ro_gain, w_out, state = args
    weights = [jnp.swapaxes(w, 2, 3) for w in (wr, wk, wv, wd, wq, wg)]
    own = tokens[0]
    rows, columns = own.shape
    head = wr.shape[3]
    layers = state.shape[0]
    flat = state.shape[3]
    planes = n // 8
    block, deep = columns // 8, 8 * rows
    bf16, f32 = jnp.bfloat16, jnp.float32
    vmem, hbm = [pl.BlockSpec(memory_space=m) for m in (pltpu.VMEM, pltpu.HBM)]
    dma = pltpu.SemaphoreType.DMA
    stay = lambda a: pltpu.with_memory_space_constraint(a, pltpu.HBM)
    operands = [own, gain, bias, self_w, ro_gain, *weights, w_out, state]
    mixed, new_state = pl.pallas_call(
        functools.partial(fused_kernel, n),
        out_shape=(
            pltpu.VMEM(own.shape, own.dtype),
            pltpu.VMEM(state.shape, state.dtype),
        ),
        in_specs=[hbm] * len(operands),
        out_specs=(vmem, vmem),
        scratch_shapes=[
            pltpu.VMEM((2 * head, flat), bf16),
            *[pltpu.VMEM(t.shape, t.dtype) for t in (gain, bias, self_w, ro_gain)],
            dma((5,)),
            pltpu.VMEM((n, rows, columns), bf16),
            pltpu.VMEM((n, 8, rows, block), bf16),
            pltpu.VMEM((layers, 6 * head, columns), bf16),
            pltpu.VMEM((layers, 8 * head, block), bf16),
            pltpu.VMEM((layers, planes, deep // 2, 2 * head), bf16),
            pltpu.VMEM((layers, planes, 8, deep // 2, 2 * head), bf16),
            pltpu.VMEM((layers, planes, deep, block), bf16),
            pltpu.VMEM((layers, planes, deep, block), bf16),
            pltpu.VMEM((planes, 8, rows, block), bf16),
            pltpu.VMEM((n, rows, block), bf16),
            pltpu.VMEM((deep, block), f32),
            dma((layers, 3)),
            dma((1,)),
            dma((5 * planes - 1,)),
            dma((layers,)),
            dma((layers,)),
            dma((planes,)),
            dma((planes,)),
            dma((layers,)),
            dma((layers,)),
            dma((1,)),
            dma((1,)),
        ],
        compiler_params=pltpu.CompilerParams(
            collective_id=0, has_side_effects=True, vmem_limit_bytes=40 << 20
        ),
        cost_estimate=pl.CostEstimate(flops=0, bytes_accessed=50 << 20, transcendentals=0),
    )(*[stay(o) for o in operands])
    held = [pltpu.with_memory_space_constraint(a, pltpu.VMEM) for a in (mixed, new_state)]
    mixed, new_state = pl.pallas_call(
        write_kernel,
        out_shape=[jax.ShapeDtypeStruct(a.shape, a.dtype) for a in held],
        in_specs=[vmem, vmem],
        out_specs=[hbm, hbm],
        scratch_shapes=[dma((1 + WRITES * layers,))],
        compiler_params=pltpu.CompilerParams(vmem_limit_bytes=1 << 20),
    )(*held)
    return mixed[None], new_state


def pick(n, *args):
    one_block = args[0].shape[2] == args[1].shape[1]
    tiles = args[0].shape[1] % 8 == 0 and args[0].shape[2] % 1024 == 0
    if one_block and tiles and n // 8 == 4 and 2 * args[2].shape[3] % 128 == 0:
        return on_device_fast(n, *args)
    return on_device(*args)


def solution(mesh):
    return jax.shard_map(
        functools.partial(pick, mesh.shape["tp"]),
        mesh=mesh,
        in_specs=(
            P("tp", None, None),
            P(),
            P(None, "tp", None, None),
            P(None, "tp", None, None),
            P(None, "tp", None, None),
            P(None, "tp", None, None),
            P(None, "tp", None, None),
            P(None, "tp", None, None),
            P(),
            P(),
            P(),
            P(None, "tp", None, None),
            P(None, "tp", None, None),
        ),
        out_specs=(P("tp", None, None), P(None, "tp", None, None)),
        check_vma=False,
    )
```
